32 devices in a mesh: sp: 8 (over z, x), tp: 4 (over y, core).
Axes of the slice: x: 2, y: 2, z: 4, core: 2. Of those that a mesh axis runs over, the one named last changes fastest.
Arguments:
- resid: bfloat16 [1024, 2048], P('sp'), may hold values from -8 to 8
- a_val: bfloat16 [1024, 1024], P('sp', 'tp'), may hold values from -8 to 8
- a_gate: bfloat16 [1024, 1024], P('sp', 'tp'), may hold values from -6 to 6
- conv_kernel: bfloat16 [31, 1024], P(None, 'tp'), may hold values from -1 to 1
- conv_bias: float32 [1024], P('tp'), may hold values from -3 to 3
- ln_gain: float32 [1024], P('tp'), may hold values from 0.1 to 1.9
- ln_bias: float32 [1024], P('tp'), may hold values from -3 to 3
- w_out: bfloat16 [1024, 2048], P('tp'), may hold values from -0.1875 to 0.1875
- ffn_gain: float32 [2048], replicated, may hold values from 0.1 to 1.9
- routes: int32 [1024, 4], P('sp'), may hold values from 0 to 7, all different within a row; in each aligned block of 128 rows (0 to 127, 128 to 255, ...) at most 128 rows name the same one
- route_weights: float32 [1024, 4], P('sp'), may hold values from 0.15 to 1.2
- exp_gate: bfloat16 [8, 2048, 4096], P('sp', None, 'tp'), may hold values from -0.125 to 0.125
- exp_up: bfloat16 [8, 2048, 4096], P('sp', None, 'tp'), may hold values from -0.125 to 0.125
- exp_down: bfloat16 [8, 4096, 2048], P('sp', None, 'tp'), may hold values from -0.09375 to 0.09375
- sh_gate: bfloat16 [2048, 512], P(None, 'tp'), may hold values from -0.125 to 0.125
- sh_up: bfloat16 [2048, 512], P(None, 'tp'), may hold values from -0.125 to 0.125
- sh_down: bfloat16 [512, 2048], P(None, 'tp'), may hold values from -0.25 to 0.25
Outputs:
- result: bfloat16 [1024, 2048], P('sp', 'tp')
The draws below stay inside these ranges and needn't reach their ends.
Inputs may be any that keep to these rules, and one draw needn't show every extreme that they name: `routes`: among the 128 rows of one index of sp, each expert is named at most 128 times, a bound that some block reaches; a row names 4 different experts.
All inputs are finite; a program needn't handle non-finite values.
Results may differ from the reference program's by a relative error of at most 0.007.
Values may be sent and summed in bfloat16 or wider, within the bound.
A program may use at most 64 MiB of HBM per device.

```python
import math
import jax
import jax.numpy as jnp
import numpy as np
from jax import lax

D = 2048
D_A = 1024
D_E = 4096
D_S = 512
CONV_SPAN = 31
TOPK = 4
TOK_SP = 128
EXPERTS = 8
TOKENS = 1024
CAP = 128
N_SP = 8


def rising_field(key, row_count, col_count, lowest, growth):
    subkeys = jax.random.split(jax.random.fold_in(key, 11), 2)
    position = jnp.arange(col_count, dtype=jnp.float32) / col_count
    roughness = jnp.exp(jax.random.uniform(subkeys[1], (col_count,), jnp.float32, -0.35, 0.35))
    values = jax.random.normal(subkeys[0], (row_count, col_count), jnp.float32)
    drawn = values * (lowest * growth ** position * roughness)[None, :]
    return jnp.clip(drawn, -8.0, 8.0)


def draw_resid(key, part):
    return rising_field(jax.random.fold_in(key, 3), TOKENS, D, 0.5, 3.0).astype(jnp.bfloat16)


def draw_a_val(key, part):
    return rising_field(jax.random.fold_in(key, 5), TOKENS, D_A, 0.5, 3.0).astype(jnp.bfloat16)


def shard_levels(rng, dims, cuts, low, top_value):
    level = 1.0
    for axis_at, shards_of in cuts:
        steps = jax.random.uniform(jax.random.fold_in(jax.random.fold_in(rng, 6), axis_at), (shards_of,), jnp.float32, low / len(cuts), top_value / len(cuts))
        level = level * jnp.repeat(jnp.exp(steps), dims[axis_at] // shards_of).reshape((-1,) + (1,) * (len(dims) - 1 - axis_at))
    return level


def deal_out(rng, own, number, rows, amount, top, limit, skew):
    order = jax.random.permutation(rng, amount)
    crowded, usual = load_shares(amount, rows * top, limit, skew, True), load_shares(amount, rows * top, limit, skew, False)
    places = jnp.arange(amount)

    def named(tallies, offset_by):
        used = int((tallies > 0).sum())
        fixed = max(1, used // 4)
        passed = fixed + (places - fixed + offset_by * (used - fixed)) % max(1, amount - fixed)
        return jnp.zeros((amount,), jnp.int32).at[order[jnp.where(places < fixed, places, passed)]].set(jnp.asarray(tallies, jnp.int32))

    tallies = jnp.where(number % 4 == 0, named(crowded, number // 4), named(usual, number - number // 4 - 1))
    mixed = jax.random.permutation(jax.random.fold_in(own, 3), amount)
    source_of, sink = mixed[0:amount // 2 * 2:2], mixed[1:amount // 2 * 2:2]
    margin = jnp.minimum(tallies[source_of] - 1, limit - tallies[sink]) // 2
    margin = jnp.where((source_of == order[0]) | (sink == order[0]) | (tallies[sink] == 0), 0, jnp.maximum(margin, 0))
    passed = jax.random.randint(jax.random.fold_in(own, 4), (amount // 2,), 0, 1 << 20) % (margin + 1)
    tallies = tallies.at[source_of].add(-passed).at[sink].add(passed)
    labels = jnp.searchsorted(jnp.cumsum(tallies), jnp.arange(rows * top), side="right").astype(jnp.int32)
    table = labels.reshape(top, rows).T
    table = table[jax.random.permutation(jax.random.fold_in(own, 1), rows)]
    offset_by = jax.random.randint(jax.random.fold_in(own, 2), (rows, 1), 0, top)
    return jnp.take_along_axis(table, (jnp.arange(top)[None, :] + offset_by) % top, axis=1)


def load_shares(count, total, limit, lean, full):
    weights = [(1 << 20) // math.isqrt(grade ** lean) + 1 for grade in range(1, count + 1)]
    largest = limit if full else min(limit, max(-(-total // count), total * weights[0] // sum(weights)))
    least = 1 if total - largest >= count - 1 else 0
    holding, spare = [largest] + [least] * (count - 1), total - largest - least * (count - 1)
    while spare > 0:
        movable = [i for i in range(1, count) if holding[i] < largest] or [i for i in range(1, count) if holding[i] < limit]
        pool, remaining = sum([weights[i] for i in movable]), spare
        for i in movable:
            addition = min(limit - holding[i], max(1, remaining * weights[i] // pool), spare)
            holding[i] = holding[i] + addition
            spare = spare - addition
    return np.array(holding)


def normal_values(key, shape, spread, limit, cuts=(), kind=jnp.bfloat16):
    values = jax.random.normal(key, shape, jnp.float32) * spread
    if len(cuts) > 0:
        values = shard_levels(key, shape, cuts, -0.22, 0.18) * values
    return jnp.clip(values, min=-limit, max=limit).astype(kind)


def setup_inputs(seed: int = 0) -> dict:
    streams_of = jax.random.split(jax.random.key(seed), 18)
    resid = draw_resid(jax.random.fold_in(streams_of[17], 71), 0)
    a_val = draw_a_val(jax.random.fold_in(streams_of[17], 71), 0)
    a_gate = normal_values(streams_of[2], (TOKENS, D_A), 1.0, 6.0, ((0, 8), (1, 4)))
    conv_kernel = normal_values(streams_of[3], (CONV_SPAN, D_A), CONV_SPAN ** -0.5, 1.0, ((1, 4),))
    conv_bias = normal_values(streams_of[4], (D_A,), 0.5, 3.0, ((0, 4),), jnp.float32)
    ln_gain = jnp.clip(1.0 + 0.18 * jax.random.normal(streams_of[5], (D_A,), jnp.float32), 0.1, 1.9)
    ln_bias = normal_values(streams_of[6], (D_A,), 0.5, 3.0, ((0, 4),), jnp.float32)
    w_out = normal_values(streams_of[7], (D_A, D), D_A ** -0.5, 0.1875, ((0, 4),))
    ffn_gain = jnp.clip(1.0 + 0.18 * jax.random.normal(streams_of[8], (D,), jnp.float32), 0.1, 1.9)
    routes_keys = jax.random.split(jax.random.fold_in(streams_of[9], 1), TOKENS // TOK_SP)
    routes_turns = jax.random.permutation(jax.random.fold_in(streams_of[9], 3), TOKENS // TOK_SP)
    routes = jax.vmap(lambda own, number: deal_out(jax.random.fold_in(streams_of[9], 2), own, number, TOK_SP, EXPERTS, TOPK, CAP, 1))(routes_keys, routes_turns).reshape((TOKENS, TOPK))
    route_weights = jnp.clip(jnp.exp(math.log(1.2) - 2.0794415 * jax.random.uniform(streams_of[10], (TOKENS, TOPK), jnp.float32) ** shard_levels(streams_of[10], (TOKENS, TOPK), ((0, 8),), -0.2, 0.2)), 0.15, 1.2)
    exp_gate = normal_values(streams_of[11], (EXPERTS, D, D_E), D ** -0.5, 0.125, ((0, 8), (2, 4)))
    exp_up = normal_values(streams_of[12], (EXPERTS, D, D_E), D ** -0.5, 0.125, ((0, 8), (2, 4)))
    exp_down = normal_values(streams_of[13], (EXPERTS, D_E, D), D_E ** -0.5, 0.09375, ((0, 8), (2, 4)))
    sh_gate = normal_values(streams_of[14], (D, D_S), D ** -0.5, 0.125, ((1, 4),))
    sh_up = normal_values(streams_of[15], (D, D_S), D ** -0.5, 0.125, ((1, 4),))
    sh_down = normal_values(streams_of[16], (D_S, D), D_S ** -0.5, 0.25, ((1, 4),))
    return dict(resid=resid, a_val=a_val, a_gate=a_gate, conv_kernel=conv_kernel, conv_bias=conv_bias, ln_gain=ln_gain, ln_bias=ln_bias, w_out=w_out, ffn_gain=ffn_gain, routes=routes, route_weights=route_weights, exp_gate=exp_gate, exp_up=exp_up, exp_down=exp_down, sh_gate=sh_gate, sh_up=sh_up, sh_down=sh_down)


LN_EPS = 1e-05
RMS_EPS = 1e-06

def reference(resid, a_val, a_gate, conv_kernel, conv_bias, ln_gain, ln_bias, w_out, ffn_gain, routes, route_weights, exp_gate, exp_up, exp_down, sh_gate, sh_up, sh_down):
    gated_in = (a_val.astype(jnp.float32) * jax.nn.sigmoid(a_gate.astype(jnp.float32))).astype(jnp.bfloat16)
    padded = jnp.pad(gated_in, ((CONV_SPAN - 1, 0), (0, 0))).astype(jnp.float32)
    kernel = conv_kernel.astype(jnp.float32)

    def add_tap(offset, running):
        window_rows = lax.dynamic_slice_in_dim(padded, offset, TOKENS, 0)
        return running + lax.dynamic_slice_in_dim(kernel, offset, 1, 0) * window_rows
    start_sum = jnp.broadcast_to(conv_bias[None, :], (TOKENS, D_A)).astype(jnp.float32)
    conv_out = lax.fori_loop(0, CONV_SPAN, add_tap, start_sum)
    channel_mean = lax.optimization_barrier(jnp.mean(conv_out, axis=1, keepdims=True))
    channel_var = lax.optimization_barrier(jnp.mean(conv_out * conv_out, axis=1, keepdims=True)) - channel_mean * channel_mean
    scaled = (conv_out - channel_mean) * lax.rsqrt(channel_var + LN_EPS) * ln_gain[None, :] + ln_bias[None, :]
    mixed_out = jax.nn.silu(scaled).astype(jnp.bfloat16)
    projected = jnp.dot(mixed_out, w_out, preferred_element_type=jnp.float32)
    middle = (resid.astype(jnp.float32) + projected).astype(jnp.bfloat16)
    middle_f = middle.astype(jnp.float32)
    inverse = lax.rsqrt(lax.optimization_barrier(jnp.mean(middle_f * middle_f, axis=1, keepdims=True)) + RMS_EPS)
    normed = (middle_f * inverse * ffn_gain[None, :]).astype(jnp.bfloat16)
    shared_gate = jnp.dot(normed, sh_gate, preferred_element_type=jnp.float32)
    shared_up = jnp.dot(normed, sh_up, preferred_element_type=jnp.float32)
    shared_hidden = (jax.nn.silu(shared_gate) * shared_up).astype(jnp.bfloat16)
    shared = jnp.dot(shared_hidden, sh_down, preferred_element_type=jnp.float32)
    pair_count = TOK_SP * TOPK
    chosen_all = routes.reshape(N_SP, pair_count)
    expert_ids = jnp.arange(EXPERTS, dtype=jnp.int32)

    def block_places(chosen):
        one_hot = (chosen[:, None] == expert_ids[None, :]).astype(jnp.int32)
        earlier = jnp.cumsum(one_hot, axis=0) - one_hot
        return lax.optimization_barrier(jnp.sum(earlier * one_hot, axis=1)).astype(jnp.int32)
    place_in = lax.map(block_places, chosen_all)
    source_ids = jnp.arange(N_SP, dtype=jnp.int32)[:, None]
    target = source_ids * (EXPERTS * CAP) + chosen_all * CAP + place_in
    pair_ids = source_ids * pair_count + jnp.arange(pair_count, dtype=jnp.int32)[None, :]
    owner_ids = jnp.zeros((N_SP * EXPERTS * CAP,), jnp.int32).at[target.reshape(-1)].set(pair_ids.reshape(-1) + 1)
    owner_ids = owner_ids.reshape(N_SP, EXPERTS, CAP).transpose(1, 0, 2)

    def run_expert(packed):
        owners, gate_weight, up_weight, down_weight = packed
        flat_owner = owners.reshape(-1)
        source_row = jnp.maximum(flat_owner - 1, 0) // TOPK
        rows_in = jnp.where((flat_owner > 0)[:, None], normed[source_row], jnp.zeros((), jnp.bfloat16))
        gate_part = jnp.dot(rows_in, gate_weight, preferred_element_type=jnp.float32)
        up_part = jnp.dot(rows_in, up_weight, preferred_element_type=jnp.float32)
        hidden = (jax.nn.silu(gate_part) * up_part).astype(jnp.bfloat16)
        return jnp.dot(hidden, down_weight, preferred_element_type=jnp.float32).astype(jnp.bfloat16)
    expert_out = lax.map(run_expert, (owner_ids, exp_gate, exp_up, exp_down))
    flat_index = (chosen_all * (N_SP * CAP) + source_ids * CAP + place_in).reshape(-1)
    flat_out = expert_out.reshape(EXPERTS * N_SP * CAP, D)
    routed = jnp.zeros((TOKENS, D), jnp.float32)
    index_grid = flat_index.reshape(TOKENS, TOPK)
    for choice_k in range(TOPK):
        picked = flat_out[index_grid[:, choice_k]].astype(jnp.float32)
        routed = routed + route_weights[:, choice_k][:, None] * picked
    return (middle_f + shared + routed).astype(jnp.bfloat16)
```

```python
import functools

import jax
import jax.numpy as jnp
from jax import lax
from jax.experimental import pallas as pl
from jax.experimental.pallas import tpu as pltpu
from jax.sharding import PartitionSpec as P

LN_EPS = 1e-05
RMS_EPS = 1e-06


def shifted(value, axis, by):
    size = lax.axis_size(axis)
    pairs = [(i, i + by) for i in range(size) if 0 <= i + by < size]
    return lax.ppermute(value, axis, pairs)


def body_slots(
    resid,
    a_val,
    a_gate,
    conv_kernel,
    conv_bias,
    ln_gain,
    ln_bias,
    w_out,
    ffn_gain,
    routes,
    route_weights,
    exp_gate,
    exp_up,
    exp_down,
    sh_gate,
    sh_up,
    sh_down,
):
    tp_count = lax.axis_size("tp")
    tp_place = lax.axis_index("tp")
    sp_count = lax.axis_size("sp")
    tok_rows = resid.shape[0]
    model_width = resid.shape[1]
    col_width = model_width // tp_count
    col_start = tp_place * col_width
    conv_span = conv_kernel.shape[0]
    channels_all = a_val.shape[1] * tp_count
    gated_in = (a_val.astype(jnp.float32) * jax.nn.sigmoid(a_gate.astype(jnp.float32))).astype(
        jnp.bfloat16
    )
    before = shifted(gated_in[tok_rows - (conv_span - 1) :], "sp", 1)
    padded = jnp.concatenate([before, gated_in], axis=0).astype(jnp.float32)
    kernel = conv_kernel.astype(jnp.float32)

    def add_tap(offset, running):
        window_rows = lax.dynamic_slice_in_dim(padded, offset, tok_rows, 0)
        return running + lax.dynamic_slice_in_dim(kernel, offset, 1, 0) * window_rows

    start_sum = jnp.broadcast_to(conv_bias[None, :], gated_in.shape)
    conv_out = lax.fori_loop(0, conv_span, add_tap, start_sum)
    row_sums = lax.psum((jnp.sum(conv_out, axis=1), jnp.sum(conv_out * conv_out, axis=1)), "tp")
    channel_mean = row_sums[0] / channels_all
    channel_var = row_sums[1] / channels_all - channel_mean * channel_mean
    scaled = (conv_out - channel_mean[:, None]) * lax.rsqrt(
        channel_var[:, None] + LN_EPS
    ) * ln_gain[None, :] + ln_bias[None, :]
    mixed_out = jax.nn.silu(scaled).astype(jnp.bfloat16)
    partial_proj = jnp.dot(mixed_out, w_out, preferred_element_type=jnp.float32)
    projected = lax.psum(partial_proj, "tp")
    middle = (resid.astype(jnp.float32) + projected).astype(jnp.bfloat16)
    middle_f = middle.astype(jnp.float32)
    inverse = lax.rsqrt(jnp.mean(middle_f * middle_f, axis=1, keepdims=True) + RMS_EPS)
    normed = (middle_f * inverse * ffn_gain[None, :]).astype(jnp.bfloat16)
    middle_cols = lax.dynamic_slice_in_dim(middle, col_start, col_width, 1)
    shared_gate = jnp.dot(normed, sh_gate, preferred_element_type=jnp.float32)
    shared_up = jnp.dot(normed, sh_up, preferred_element_type=jnp.float32)
    shared_hidden = (jax.nn.silu(shared_gate) * shared_up).astype(jnp.bfloat16)
    weight_rows = sh_down
    shared = jnp.dot(
        lax.all_gather(shared_hidden, "tp", axis=1, tiled=True),
        weight_rows,
        preferred_element_type=jnp.float32,
    )
    top_count = routes.shape[1]
    local_experts = exp_gate.shape[0]
    experts_all = local_experts * sp_count
    capacity = max(2 * tok_rows * top_count // experts_all, tp_count)
    pair_count = tok_rows * top_count
    chosen = routes.reshape(pair_count)
    one_hot = (chosen[:, None] == jnp.arange(experts_all, dtype=jnp.int32)[None, :]).astype(
        jnp.int32
    )
    earlier = jnp.cumsum(one_hot, axis=0) - one_hot
    place_in = jnp.sum(earlier * one_hot, axis=1)
    slot_of = chosen * capacity + place_in
    owner_ids = (
        jnp.zeros((experts_all * capacity,), jnp.int32)
        .at[slot_of]
        .set(jnp.arange(pair_count, dtype=jnp.int32) + 1)
    )
    owner_grid = owner_ids.reshape(sp_count, local_experts, capacity)
    part_slots = capacity // tp_count
    own_owners = lax.dynamic_slice_in_dim(owner_grid, tp_place * part_slots, part_slots, 2)
    source_row = jnp.maximum(own_owners - 1, 0) // top_count
    taken = normed[source_row.reshape(-1)].reshape(own_owners.shape + (model_width,))
    landed = lax.all_to_all(
        jnp.where((own_owners > 0)[..., None], taken, jnp.zeros((), jnp.bfloat16)),
        "sp",
        split_axis=0,
        concat_axis=0,
        tiled=True,
    )
    arrived = lax.all_gather(landed, "tp", axis=2, tiled=True)
    gate_part = jnp.einsum("sxcd,xdf->sxcf", arrived, exp_gate, preferred_element_type=jnp.float32)
    up_part = jnp.einsum("sxcd,xdf->sxcf", arrived, exp_up, preferred_element_type=jnp.float32)
    expert_hidden = (jax.nn.silu(gate_part) * up_part).astype(jnp.bfloat16)
    weight_rows = exp_down
    expert_sum = jnp.einsum(
        "sxcf,xfd->sxcd",
        lax.all_gather(expert_hidden, "tp", axis=3, tiled=True),
        weight_rows,
        preferred_element_type=jnp.float32,
    )
    expert_out = expert_sum.astype(jnp.bfloat16)
    returned = lax.all_to_all(expert_out, "sp", split_axis=0, concat_axis=0, tiled=True)
    flat_out = returned.reshape(experts_all * capacity, col_width)
    picked = flat_out[slot_of].astype(jnp.float32).reshape(tok_rows, top_count, col_width)
    routed = jnp.sum(picked * route_weights[:, :, None], axis=1)
    return (middle_cols.astype(jnp.float32) + shared + routed).astype(jnp.bfloat16)


ROW_CUTS = 2


def silu(value):
    return value / (1.0 + jnp.exp(-value))


def layer_kernel(
    levels,
    resid_hbm,
    a_val_hbm,
    a_gate_hbm,
    taps_hbm,
    conv_bias_hbm,
    ln_gain_hbm,
    ln_bias_hbm,
    w_out_hbm,
    ffn_gain_hbm,
    routes_ref,
    route_weights_ref,
    exp_gate_hbm,
    exp_up_hbm,
    exp_down_hbm,
    sh_gate_hbm,
    sh_up_hbm,
    sh_down_hbm,
    out_ref,
    resid_ref,
    a_val_ref,
    a_gate_ref,
    taps_ref,
    conv_bias_ref,
    ln_gain_ref,
    ln_bias_ref,
    w_out_ref,
    ffn_gain_ref,
    gate_ref,
    up_ref,
    down_ref,
    sh_gate_ref,
    sh_up_ref,
    sh_down_ref,
    halo_out,
    halo_in,
    padded_ref,
    conv_ref,
    stat_out,
    stat_in,
    give_out,
    give_in,
    keep_ref,
    chip_out,
    chip_in,
    rows_ref,
    normed_ref,
    hidden_ref,
    shared_ref,
    part_ref,
    back_ref,
    load_sem,
    halo_sem,
    stat_send,
    stat_recv,
    give_send,
    give_recv,
    chip_send,
    chip_recv,
    up_sem,
    low_sem,
    side_sem,
    core_sem,
    main_recv,
    core_recv,
    far_send,
    far_recv,
    near_send,
    near_recv,
    relay_send,
    relay_recv,
    shared_send,
    shared_recv,
    back_send,
    back_recv,
):
    count = 2 * levels
    me = lax.axis_index("sp")
    tp_place = lax.axis_index("tp")
    level, side = me // 2, me % 2
    row, core = tp_place // 2, tp_place % 2
    core_place = row * 2 + (1 - core)
    row_place = (1 - row) * 2 + core
    core_peer = {"tp": core_place}
    row_peer = {"tp": row_place}
    far_peer = {"tp": (1 - row) * 2 + (1 - core)}
    side_peer = {"sp": level * 2 + (1 - side)}
    mesh_ids = pl.DeviceIdType.MESH
    f32, bf16 = jnp.float32, jnp.bfloat16
    tok_rows, half_width = resid_ref.shape
    model_width = 2 * half_width
    col_width = out_ref.shape[1]
    span = taps_ref.shape[0]
    halo_rows = halo_in.shape[0]
    channels_all = 4 * a_val_ref.shape[1]
    part_hidden = gate_ref.shape[1]
    cut_rows = tok_rows // ROW_CUTS

    half_at = pl.ds(pl.multiple_of(core * half_width, half_width), half_width)
    pairs = [
        (a_val_hbm, a_val_ref),
        (a_gate_hbm, a_gate_ref),
        (taps_hbm, taps_ref),
        (conv_bias_hbm, conv_bias_ref),
        (ln_gain_hbm, ln_gain_ref),
        (ln_bias_hbm, ln_bias_ref),
        (w_out_hbm, w_out_ref),
        (resid_hbm.at[:, half_at], resid_ref),
        (ffn_gain_hbm, ffn_gain_ref),
        (exp_gate_hbm, gate_ref),
        (exp_up_hbm, up_ref),
        (sh_gate_hbm, sh_gate_ref),
        (sh_up_hbm, sh_up_ref),
        (exp_down_hbm, down_ref),
        (sh_down_hbm, sh_down_ref),
    ]
    loads = [
        pltpu.make_async_copy(src, dst, load_sem.at[at]) for at, (src, dst) in enumerate(pairs)
    ]
    for load in loads:
        load.start()

    barrier = pltpu.get_barrier_semaphore()
    others = [lax.rem(me + step, count) for step in range(1, count)]
    for other in others:
        pl.semaphore_signal(barrier, inc=1, device_id={"sp": other}, device_id_type=mesh_ids)
    for peer in (core_peer, row_peer, far_peer):
        pl.semaphore_signal(barrier, inc=1, device_id=peer, device_id_type=mesh_ids)

    def remote(src, dst, send, recv, where):
        return pltpu.make_async_remote_copy(
            src_ref=src, dst_ref=dst, send_sem=send, recv_sem=recv, device_id=where, device_id_type=mesh_ids
        )

    for load in loads[:4]:
        load.wait()
    gated = (a_val_ref[...].astype(f32) / (1.0 + jnp.exp(-a_gate_ref[...].astype(f32)))).astype(bf16)
    halo_out[...] = gated[tok_rows - halo_rows :]
    padded_ref[halo_rows:, :] = gated.astype(f32)
    taps = taps_ref[...].astype(f32)

    def convolve(first, size):
        total = jnp.broadcast_to(conv_bias_ref[...], (size, gated.shape[1]))
        for tap in range(span):
            at = first + tap + halo_rows - (span - 1)
            total = total + taps[tap : tap + 1] * padded_ref[at : at + size, :]
        conv_ref[first : first + size, :] = total

    pl.semaphore_wait(barrier, count + 2)
    halo = lambda where: remote(halo_out, halo_in, halo_sem.at[0], halo_sem.at[1], {"sp": where})

    @pl.when(me < count - 1)
    def _():
        halo(me + 1).start()

    convolve(halo_rows, tok_rows - halo_rows)

    @pl.when(me == 0)
    def _():
        padded_ref[:halo_rows, :] = jnp.zeros((halo_rows, gated.shape[1]), f32)

    @pl.when(me > 0)
    def _():
        halo(me).wait_recv()
        padded_ref[:halo_rows, :] = halo_in[...].astype(f32)

    convolve(0, halo_rows)

    conv_out = conv_ref[...]
    diagonal = lax.broadcasted_iota(jnp.int32, (tok_rows, tok_rows), 0) == lax.broadcasted_iota(
        jnp.int32, (tok_rows, tok_rows), 1
    )

    def lying(column):
        return jnp.sum(jnp.where(diagonal, column, 0.0), axis=0, keepdims=True)

    def standing(line):
        return jnp.sum(jnp.where(diagonal, line, 0.0), axis=1, keepdims=True)

    stat_out[0:1, :] = lying(jnp.sum(conv_out, axis=1, keepdims=True))
    stat_out[1:2, :] = lying(jnp.sum(conv_out * conv_out, axis=1, keepdims=True))
    stats = [
        remote(stat_out, stat_in.at[at], stat_send.at[at], stat_recv.at[at], peer)
        for at, peer in enumerate((core_peer, row_peer, far_peer))
    ]
    for copy in stats:
        copy.start()
    for load in loads[4:9]:
        load.wait()
    for copy in stats:
        copy.wait_recv()
    sums = (stat_out[...] + stat_in[0]) + (stat_in[1] + stat_in[2])
    channel_mean = standing(sums[0:1]) / channels_all
    channel_var = standing(sums[1:2]) / channels_all - channel_mean * channel_mean
    scaled = (conv_out - channel_mean) * lax.rsqrt(channel_var + LN_EPS) * ln_gain_ref[
        ...
    ] + ln_bias_ref[...]
    mixed = silu(scaled).astype(bf16)

    give_at = pl.ds(pl.multiple_of((1 - core) * half_width, half_width), half_width)
    give_out[...] = jnp.dot(mixed, w_out_ref[:, give_at], preferred_element_type=f32).astype(bf16)

    def cut(at):
        return pl.ds(at * cut_rows, cut_rows)

    gives = [
        remote(
            give_out.at[cut(at)], give_in.at[cut(at)], give_send.at[at], give_recv.at[at], core_peer
        )
        for at in range(ROW_CUTS)
    ]
    for copy in gives:
        copy.start()
    keep_ref[...] = jnp.dot(mixed, w_out_ref[:, half_at], preferred_element_type=f32)
    chips = [
        remote(
            chip_out.at[cut(at)], chip_in.at[cut(at)], chip_send.at[at], chip_recv.at[at], row_peer
        )
        for at in range(ROW_CUTS)
    ]
    for at in range(ROW_CUTS):
        gives[at].wait_recv()
        chip_sum = keep_ref[cut(at), :] + give_in[cut(at), :].astype(f32)
        keep_ref[cut(at), :] = chip_sum
        chip_out[cut(at), :] = chip_sum.astype(bf16)
        chips[at].start()

    def block(half, at, piece):
        return rows_ref.at[half, at, cut(piece)]

    def up_copy(origin, piece):
        at = origin * 2 + side
        sem = origin * ROW_CUTS + piece
        spot = block(core, at, piece)
        return remote(spot, spot, up_sem.at[sem], main_recv.at[at * ROW_CUTS + piece], {"sp": me + 2})

    def low_copy(origin, piece):
        at = origin * 2 + side
        sem = origin * ROW_CUTS + piece
        spot = block(core, at, piece)
        return remote(spot, spot, low_sem.at[sem], main_recv.at[at * ROW_CUTS + piece], {"sp": me - 2})

    def side_copy(origin, piece):
        at = origin * 2 + side
        sem = origin * ROW_CUTS + piece
        spot = block(core, at, piece)
        return remote(spot, spot, side_sem.at[sem], main_recv.at[at * ROW_CUTS + piece], side_peer)

    def core_copy(at, piece):
        sem = at * ROW_CUTS + piece
        spot = block(core, at, piece)
        return remote(spot, spot, core_sem.at[sem], core_recv.at[sem], core_peer)

    def landed(at, piece):
        spot = block(core, at, piece)
        sem = at * ROW_CUTS + piece
        remote(spot, spot, core_sem.at[sem], main_recv.at[sem], core_peer).wait_recv()

    def crossed(at, piece):
        spot = block(1 - core, at, piece)
        sem = at * ROW_CUTS + piece
        remote(spot, spot, core_sem.at[sem], core_recv.at[sem], core_peer).wait_recv()

    for at in range(ROW_CUTS):
        chips[at].wait_recv()
        total = keep_ref[cut(at), :] + chip_in[cut(at), :].astype(f32)
        rows_ref[core, me, cut(at), :] = (resid_ref[cut(at), :].astype(f32) + total).astype(bf16)
        core_copy(me, at).start()
        side_copy(level, at).start()

        @pl.when(level < levels - 1)
        def _():
            up_copy(level, at).start()

        @pl.when(level > 0)
        def _():
            low_copy(level, at).start()

    def normalise(at):
        low = rows_ref[0, at].astype(f32)
        high = rows_ref[1, at].astype(f32)
        power = jnp.sum(low * low, axis=1, keepdims=True) + jnp.sum(high * high, axis=1, keepdims=True)
        inverse = lax.rsqrt(power / model_width + RMS_EPS)
        normed_ref[:, :half_width] = (low * inverse * ffn_gain_ref[:, :half_width]).astype(bf16)
        normed_ref[:, half_width:] = (high * inverse * ffn_gain_ref[:, half_width:]).astype(bf16)

    def far_copy(at):
        spot = hidden_ref.at[tp_place, at]
        return remote(spot, spot, far_send.at[at], far_recv.at[at], row_peer)

    def near_copy(at):
        spot = hidden_ref.at[tp_place, at]
        return remote(spot, spot, near_send.at[at], near_recv.at[at], core_peer)

    def relay_copy(at):
        spot = hidden_ref.at[row_place, at]
        return remote(spot, spot, relay_send.at[at], relay_recv.at[at], core_peer)

    shared_far = remote(
        shared_ref.at[tp_place], shared_ref.at[tp_place], shared_send.at[0], shared_recv.at[0], row_peer
    )
    shared_near = remote(
        shared_ref.at[tp_place], shared_ref.at[tp_place], shared_send.at[1], shared_recv.at[1], core_peer
    )
    shared_relay = remote(
        shared_ref.at[row_place], shared_ref.at[row_place], shared_send.at[2], shared_recv.at[2], core_peer
    )

    def hide(at):
        for piece in range(ROW_CUTS):
            crossed(at, piece)
        normalise(at)
        step = 256
        for first in range(0, part_hidden, step):
            wide = slice(first, first + step)
            gate_part = jnp.dot(normed_ref[...], gate_ref[:, wide], preferred_element_type=f32)
            up_part = jnp.dot(normed_ref[...], up_ref[:, wide], preferred_element_type=f32)
            hidden_ref[tp_place, at, :, wide] = (silu(gate_part) * up_part).astype(bf16)
        far_copy(at).start()
        near_copy(at).start()

    def back_copy(at):
        return remote(part_ref.at[at], back_ref.at[me], back_send.at[at], back_recv.at[me], {"sp": at})

    def finish(at):
        far_copy(at).wait_recv()
        relay_copy(at).start()
        near_copy(at).wait_recv()
        relay_copy(at).wait_recv()
        total = jnp.zeros((tok_rows, col_width), f32)
        for place in range(4):
            total = total + jnp.dot(
                hidden_ref[place, at],
                down_ref[place * part_hidden : (place + 1) * part_hidden, :],
                preferred_element_type=f32,
            )
        result = total.astype(bf16)

        @pl.when(at == me)
        def _():
            back_ref[me] = result

        @pl.when(at != me)
        def _():
            part_ref[at] = result
            back_copy(at).start()

    turn = 1 - 2 * ((2 * level) // levels)

    def level_at(step):
        return lax.rem(level + turn * step + levels, levels)

    for load in loads[9:13]:
        load.wait()
    hide(me)
    shared_gate = jnp.dot(normed_ref[...], sh_gate_ref[...], preferred_element_type=f32)
    shared_up = jnp.dot(normed_ref[...], sh_up_ref[...], preferred_element_type=f32)
    shared_ref[tp_place] = (silu(shared_gate) * shared_up).astype(bf16)
    shared_far.start()
    shared_near.start()
    for load in loads[13:]:
        load.wait()

    def pass_on(step):
        below = level - step
        above = level + step

        @pl.when(below >= 0)
        def _():
            for piece in range(ROW_CUTS):
                landed(below * 2 + side, piece)
                core_copy(below * 2 + side, piece).start()
                side_copy(below, piece).start()

                @pl.when(level < levels - 1)
                def _():
                    up_copy(below, piece).start()

        @pl.when(above < levels)
        def _():
            for piece in range(ROW_CUTS):
                landed(above * 2 + side, piece)
                core_copy(above * 2 + side, piece).start()
                side_copy(above, piece).start()

                @pl.when(level > 0)
                def _():
                    low_copy(above, piece).start()

    def visit(step, before):
        near_level = level_at(step)
        own = near_level * 2 + side
        other = near_level * 2 + (1 - side)

        @pl.when(step > 0)
        def _():
            hide(own)
            finish(before)

        for piece in range(ROW_CUTS):
            landed(other, piece)
            core_copy(other, piece).start()

        @pl.when(step < levels - 1)
        def _():
            pass_on(step + 1)

        hide(other)
        finish(own)
        return other

    last = lax.fori_loop(0, levels, visit, me)
    finish(last)

    middle_cols = rows_ref[row, me, :, pl.ds(pl.multiple_of(core * col_width, col_width), col_width)]
    shared_far.wait_recv()
    shared_relay.start()
    shared_near.wait_recv()
    shared_relay.wait_recv()
    total = middle_cols.astype(f32)
    shared_width = shared_ref.shape[2]
    for place in range(4):
        total = total + jnp.dot(
            shared_ref[place],
            sh_down_ref[place * shared_width : (place + 1) * shared_width, :],
            preferred_element_type=f32,
        )
    routes = routes_ref[...]
    route_weights = route_weights_ref[...]
    for at in range(count):

        @pl.when(me != at)
        def _():
            remote(
                part_ref.at[at], back_ref.at[at], back_send.at[at], back_recv.at[at], core_peer
            ).wait_recv()

        weight = jnp.sum(jnp.where(routes == at, route_weights, 0.0), axis=1, keepdims=True)
        total = total + weight * back_ref[at].astype(f32)
    out_ref[...] = total.astype(bf16)

    @pl.when(me < count - 1)
    def _():
        halo(me + 1).wait_send()

    for copy in stats + gives + chips + [shared_far, shared_near, shared_relay]:
        copy.wait_send()

    @pl.loop(0, levels)
    def _(origin):
        for piece in range(ROW_CUTS):
            side_copy(origin, piece).wait_send()

            @pl.when((level < levels - 1) & (origin <= level))
            def _():
                up_copy(origin, piece).wait_send()

            @pl.when((level > 0) & (origin >= level))
            def _():
                low_copy(origin, piece).wait_send()

    @pl.loop(0, count)
    def _(at):
        for piece in range(ROW_CUTS):
            core_copy(at, piece).wait_send()
        far_copy(at).wait_send()
        near_copy(at).wait_send()
        relay_copy(at).wait_send()

        @pl.when(at != me)
        def _():
            back_copy(at).wait_send()


def body_dense(
    resid,
    a_val,
    a_gate,
    conv_kernel,
    conv_bias,
    ln_gain,
    ln_bias,
    w_out,
    ffn_gain,
    routes,
    route_weights,
    exp_gate,
    exp_up,
    exp_down,
    sh_gate,
    sh_up,
    sh_down,
):
    count = lax.axis_size("sp")
    levels = count // 2
    tok_rows, model_width = resid.shape
    half_width = model_width // 2
    channels = a_val.shape[1]
    part_hidden = exp_gate.shape[2]
    col_width = exp_down.shape[2]
    shared_width = sh_gate.shape[1]
    span = conv_kernel.shape[0]
    halo_rows = -(-(span - 1) // 16) * 16
    vmem = pl.BlockSpec(memory_space=pltpu.VMEM)
    hbm = pl.BlockSpec(memory_space=pltpu.HBM)
    f32, bf16 = jnp.float32, jnp.bfloat16
    dma = pltpu.SemaphoreType.DMA
    operands = (
        resid,
        a_val,
        a_gate,
        conv_kernel,
        conv_bias.reshape(1, -1),
        ln_gain.reshape(1, -1),
        ln_bias.reshape(1, -1),
        w_out,
        ffn_gain.reshape(1, -1),
        routes,
        route_weights,
        exp_gate[0],
        exp_up[0],
        exp_down[0],
        sh_gate,
        sh_up,
        sh_down,
    )
    pieces = count * ROW_CUTS
    return pl.pallas_call(
        functools.partial(layer_kernel, levels),
        out_shape=jax.ShapeDtypeStruct((tok_rows, col_width), bf16),
        in_specs=[hbm] * 9 + [vmem] * 2 + [hbm] * 6,
        out_specs=vmem,
        scratch_shapes=[
            pltpu.VMEM((tok_rows, half_width), bf16),
            pltpu.VMEM(a_val.shape, bf16),
            pltpu.VMEM(a_gate.shape, bf16),
            pltpu.VMEM(conv_kernel.shape, bf16),
            pltpu.VMEM((1, channels), f32),
            pltpu.VMEM((1, channels), f32),
            pltpu.VMEM((1, channels), f32),
            pltpu.VMEM(w_out.shape, bf16),
            pltpu.VMEM((1, model_width), f32),
            pltpu.VMEM(exp_gate.shape[1:], bf16),
            pltpu.VMEM(exp_up.shape[1:], bf16),
            pltpu.VMEM(exp_down.shape[1:], bf16),
            pltpu.VMEM(sh_gate.shape, bf16),
            pltpu.VMEM(sh_up.shape, bf16),
            pltpu.VMEM(sh_down.shape, bf16),
            pltpu.VMEM((halo_rows, channels), bf16),
            pltpu.VMEM((halo_rows, channels), bf16),
            pltpu.VMEM((halo_rows + tok_rows, channels), f32),
            pltpu.VMEM((tok_rows, channels), f32),
            pltpu.VMEM((2, tok_rows), f32),
            pltpu.VMEM((3, 2, tok_rows), f32),
            pltpu.VMEM((tok_rows, half_width), bf16),
            pltpu.VMEM((tok_rows, half_width), bf16),
            pltpu.VMEM((tok_rows, half_width), f32),
            pltpu.VMEM((tok_rows, half_width), bf16),
            pltpu.VMEM((tok_rows, half_width), bf16),
            pltpu.VMEM((2, count, tok_rows, half_width), bf16),
            pltpu.VMEM((tok_rows, model_width), bf16),
            pltpu.VMEM((4, count, tok_rows, part_hidden), bf16),
            pltpu.VMEM((4, tok_rows, shared_width), bf16),
            pltpu.VMEM((count, tok_rows, col_width), bf16),
            pltpu.VMEM((count, tok_rows, col_width), bf16),
            dma((15,)),
            dma((2,)),
            dma((3,)),
            dma((3,)),
            dma((ROW_CUTS,)),
            dma((ROW_CUTS,)),
            dma((ROW_CUTS,)),
            dma((ROW_CUTS,)),
            dma((levels * ROW_CUTS,)),
            dma((levels * ROW_CUTS,)),
            dma((levels * ROW_CUTS,)),
            dma((pieces,)),
            dma((pieces,)),
            dma((pieces,)),
            dma((count,)),
            dma((count,)),
            dma((count,)),
            dma((count,)),
            dma((count,)),
            dma((count,)),
            dma((3,)),
            dma((3,)),
            dma((count,)),
            dma((count,)),
        ],
        compiler_params=pltpu.CompilerParams(
            collective_id=0, has_side_effects=True, vmem_limit_bytes=56 * 1024 * 1024
        ),
    )(*operands)


def body(*args):
    tok_rows = args[0].shape[0]
    top_count = args[9].shape[1]
    local_experts = args[11].shape[0]
    experts_all = local_experts * lax.axis_size("sp")
    capacity = 2 * tok_rows * top_count // experts_all
    if (
        local_experts == 1
        and lax.axis_size("tp") == 4
        and lax.axis_size("sp") % 2 == 0
        and capacity >= tok_rows
    ):
        return body_dense(*args)
    return body_slots(*args)


def solution(mesh):
    in_specs = (
        P("sp", None),
        P("sp", "tp"),
        P("sp", "tp"),
        P(None, "tp"),
        P("tp"),
        P("tp"),
        P("tp"),
        P("tp", None),
        P(),
        P("sp", None),
        P("sp", None),
        P("sp", None, "tp"),
        P("sp", None, "tp"),
        P("sp", None, "tp"),
        P(None, "tp"),
        P(None, "tp"),
        P(None, "tp"),
    )
    out_specs = P("sp", "tp")
    return jax.shard_map(body, mesh=mesh, in_specs=in_specs, out_specs=out_specs, check_vma=False)
```

```python
import functools

import jax
import jax.numpy as jnp
from jax import lax
from jax.experimental import pallas as pl
from jax.experimental.pallas import tpu as pltpu
from jax.sharding import PartitionSpec as P

LN_EPS = 1e-05
RMS_EPS = 1e-06


def shifted(value, axis, by):
    size = lax.axis_size(axis)
    pairs = [(i, i + by) for i in range(size) if 0 <= i + by < size]
    return lax.ppermute(value, axis, pairs)


def body_slots(
    resid,
    a_val,
    a_gate,
    conv_kernel,
    conv_bias,
    ln_gain,
    ln_bias,
    w_out,
    ffn_gain,
    routes,
    route_weights,
    exp_gate,
    exp_up,
    exp_down,
    sh_gate,
    sh_up,
    sh_down,
):
    tp_count = lax.axis_size("tp")
    tp_place = lax.axis_index("tp")
    sp_count = lax.axis_size("sp")
    tok_rows = resid.shape[0]
    model_width = resid.shape[1]
    col_width = model_width // tp_count
    col_start = tp_place * col_width
    conv_span = conv_kernel.shape[0]
    channels_all = a_val.shape[1] * tp_count
    gated_in = (a_val.astype(jnp.float32) * jax.nn.sigmoid(a_gate.astype(jnp.float32))).astype(
        jnp.bfloat16
    )
    before = shifted(gated_in[tok_rows - (conv_span - 1) :], "sp", 1)
    padded = jnp.concatenate([before, gated_in], axis=0).astype(jnp.float32)
    kernel = conv_kernel.astype(jnp.float32)

    def add_tap(offset, running):
        window_rows = lax.dynamic_slice_in_dim(padded, offset, tok_rows, 0)
        return running + lax.dynamic_slice_in_dim(kernel, offset, 1, 0) * window_rows

    start_sum = jnp.broadcast_to(conv_bias[None, :], gated_in.shape)
    conv_out = lax.fori_loop(0, conv_span, add_tap, start_sum)
    row_sums = lax.psum((jnp.sum(conv_out, axis=1), jnp.sum(conv_out * conv_out, axis=1)), "tp")
    channel_mean = row_sums[0] / channels_all
    channel_var = row_sums[1] / channels_all - channel_mean * channel_mean
    scaled = (conv_out - channel_mean[:, None]) * lax.rsqrt(
        channel_var[:, None] + LN_EPS
    ) * ln_gain[None, :] + ln_bias[None, :]
    mixed_out = jax.nn.silu(scaled).astype(jnp.bfloat16)
    partial_proj = jnp.dot(mixed_out, w_out, preferred_element_type=jnp.float32)
    projected = lax.psum(partial_proj, "tp")
    middle = (resid.astype(jnp.float32) + projected).astype(jnp.bfloat16)
    middle_f = middle.astype(jnp.float32)
    inverse = lax.rsqrt(jnp.mean(middle_f * middle_f, axis=1, keepdims=True) + RMS_EPS)
    normed = (middle_f * inverse * ffn_gain[None, :]).astype(jnp.bfloat16)
    middle_cols = lax.dynamic_slice_in_dim(middle, col_start, col_width, 1)
    shared_gate = jnp.dot(normed, sh_gate, preferred_element_type=jnp.float32)
    shared_up = jnp.dot(normed, sh_up, preferred_element_type=jnp.float32)
    shared_hidden = (jax.nn.silu(shared_gate) * shared_up).astype(jnp.bfloat16)
    weight_rows = sh_down
    shared = jnp.dot(
        lax.all_gather(shared_hidden, "tp", axis=1, tiled=True),
        weight_rows,
        preferred_element_type=jnp.float32,
    )
    top_count = routes.shape[1]
    local_experts = exp_gate.shape[0]
    experts_all = local_experts * sp_count
    capacity = max(2 * tok_rows * top_count // experts_all, tp_count)
    pair_count = tok_rows * top_count
    chosen = routes.reshape(pair_count)
    one_hot = (chosen[:, None] == jnp.arange(experts_all, dtype=jnp.int32)[None, :]).astype(
        jnp.int32
    )
    earlier = jnp.cumsum(one_hot, axis=0) - one_hot
    place_in = jnp.sum(earlier * one_hot, axis=1)
    slot_of = chosen * capacity + place_in
    owner_ids = (
        jnp.zeros((experts_all * capacity,), jnp.int32)
        .at[slot_of]
        .set(jnp.arange(pair_count, dtype=jnp.int32) + 1)
    )
    owner_grid = owner_ids.reshape(sp_count, local_experts, capacity)
    part_slots = capacity // tp_count
    own_owners = lax.dynamic_slice_in_dim(owner_grid, tp_place * part_slots, part_slots, 2)
    source_row = jnp.maximum(own_owners - 1, 0) // top_count
    taken = normed[source_row.reshape(-1)].reshape(own_owners.shape + (model_width,))
    landed = lax.all_to_all(
        jnp.where((own_owners > 0)[..., None], taken, jnp.zeros((), jnp.bfloat16)),
        "sp",
        split_axis=0,
        concat_axis=0,
        tiled=True,
    )
    arrived = lax.all_gather(landed, "tp", axis=2, tiled=True)
    gate_part = jnp.einsum("sxcd,xdf->sxcf", arrived, exp_gate, preferred_element_type=jnp.float32)
    up_part = jnp.einsum("sxcd,xdf->sxcf", arrived, exp_up, preferred_element_type=jnp.float32)
    expert_hidden = (jax.nn.silu(gate_part) * up_part).astype(jnp.bfloat16)
    weight_rows = exp_down
    expert_sum = jnp.einsum(
        "sxcf,xfd->sxcd",
        lax.all_gather(expert_hidden, "tp", axis=3, tiled=True),
        weight_rows,
        preferred_element_type=jnp.float32,
    )
    expert_out = expert_sum.astype(jnp.bfloat16)
    returned = lax.all_to_all(expert_out, "sp", split_axis=0, concat_axis=0, tiled=True)
    flat_out = returned.reshape(experts_all * capacity, col_width)
    picked = flat_out[slot_of].astype(jnp.float32).reshape(tok_rows, top_count, col_width)
    routed = jnp.sum(picked * route_weights[:, :, None], axis=1)
    return (middle_cols.astype(jnp.float32) + shared + routed).astype(jnp.bfloat16)


ROW_CUTS = 2


def silu(value):
    return value / (1.0 + jnp.exp(-value))


def layer_kernel(
    levels,
    resid_hbm,
    a_val_hbm,
    a_gate_hbm,
    taps_hbm,
    conv_bias_hbm,
    ln_gain_hbm,
    ln_bias_hbm,
    w_out_hbm,
    ffn_gain_hbm,
    routes_hbm,
    route_weights_hbm,
    exp_gate_hbm,
    exp_up_hbm,
    exp_down_hbm,
    sh_gate_hbm,
    sh_up_hbm,
    sh_down_hbm,
    out_ref,
    resid_ref,
    a_val_ref,
    a_gate_ref,
    taps_ref,
    conv_bias_ref,
    ln_gain_ref,
    ln_bias_ref,
    w_out_ref,
    ffn_gain_ref,
    routes_ref,
    route_weights_ref,
    gate_ref,
    up_ref,
    down_ref,
    sh_gate_ref,
    sh_up_ref,
    sh_down_ref,
    halo_out,
    halo_in,
    padded_ref,
    conv_ref,
    stat_out,
    stat_in,
    give_out,
    give_in,
    keep_ref,
    chip_out,
    chip_in,
    rows_ref,
    normed_ref,
    hidden_ref,
    shared_ref,
    part_ref,
    back_ref,
    sum_ref,
    load_sem,
    halo_sem,
    stat_send,
    stat_recv,
    give_send,
    give_recv,
    chip_send,
    chip_recv,
    up_sem,
    low_sem,
    side_sem,
    core_sem,
    main_recv,
    core_recv,
    far_send,
    far_recv,
    near_send,
    near_recv,
    relay_send,
    relay_recv,
    shared_send,
    shared_recv,
    back_send,
    back_recv,
):
    count = 2 * levels
    me = lax.axis_index("sp")
    tp_place = lax.axis_index("tp")
    level, side = me // 2, me % 2
    row, core = tp_place // 2, tp_place % 2
    core_place = row * 2 + (1 - core)
    row_place = (1 - row) * 2 + core
    core_peer = {"tp": core_place}
    row_peer = {"tp": row_place}
    far_peer = {"tp": (1 - row) * 2 + (1 - core)}
    side_peer = {"sp": level * 2 + (1 - side)}
    mesh_ids = pl.DeviceIdType.MESH
    f32, bf16 = jnp.float32, jnp.bfloat16
    tok_rows, half_width = resid_ref.shape
    model_width = 2 * half_width
    col_width = out_ref.shape[1]
    span = taps_ref.shape[0]
    halo_rows = halo_in.shape[0]
    channels_all = 4 * a_val_ref.shape[1]
    part_hidden = gate_ref.shape[1]
    cut_rows = tok_rows // ROW_CUTS

    half_at = pl.ds(pl.multiple_of(core * half_width, half_width), half_width)
    pairs = [
        (a_val_hbm, a_val_ref),
        (a_gate_hbm, a_gate_ref),
        (taps_hbm, taps_ref),
        (conv_bias_hbm, conv_bias_ref),
        (ln_gain_hbm, ln_gain_ref),
        (ln_bias_hbm, ln_bias_ref),
        (w_out_hbm, w_out_ref),
        (resid_hbm.at[:, half_at], resid_ref),
        (ffn_gain_hbm, ffn_gain_ref),
        (exp_gate_hbm, gate_ref),
        (exp_up_hbm, up_ref),
        (sh_gate_hbm, sh_gate_ref),
        (sh_up_hbm, sh_up_ref),
        (exp_down_hbm, down_ref),
        (sh_down_hbm, sh_down_ref),
        (routes_hbm, routes_ref),
        (route_weights_hbm, route_weights_ref),
    ]
    loads = [
        pltpu.make_async_copy(src, dst, load_sem.at[at]) for at, (src, dst) in enumerate(pairs)
    ]
    for load in loads:
        load.start()

    barrier = pltpu.get_barrier_semaphore()

    def greet(peer):
        pl.semaphore_signal(barrier, inc=1, device_id=peer, device_id_type=mesh_ids)

    across = ((side == 0) & (level > 0)) | ((side == 1) & (level < levels - 1))
    for peer in (core_peer, row_peer, far_peer, side_peer):
        greet(peer)

    @pl.when(level > 0)
    def _():
        greet({"sp": me - 2})

    @pl.when(level < levels - 1)
    def _():
        greet({"sp": me + 2})

    @pl.when(across)
    def _():
        greet({"sp": me + 2 * side - 1})

    def remote(src, dst, send, recv, where):
        return pltpu.make_async_remote_copy(
            src_ref=src, dst_ref=dst, send_sem=send, recv_sem=recv, device_id=where, device_id_type=mesh_ids
        )

    for load in loads[:4]:
        load.wait()
    gated = (a_val_ref[...].astype(f32) / (1.0 + jnp.exp(-a_gate_ref[...].astype(f32)))).astype(bf16)
    halo_out[...] = gated[tok_rows - halo_rows :]
    padded_ref[halo_rows:, :] = gated.astype(f32)
    taps = taps_ref[...].astype(f32)

    def convolve(first, size):
        total = jnp.broadcast_to(conv_bias_ref[...], (size, gated.shape[1]))
        for tap in range(span):
            at = first + tap + halo_rows - (span - 1)
            total = total + taps[tap : tap + 1] * padded_ref[at : at + size, :]
        conv_ref[first : first + size, :] = total

    has_below = (level + levels - 2) // (levels - 1)
    has_above = (2 * levels - 3 - level) // (levels - 1)
    has_across = has_below + side * (has_above - has_below)
    pl.semaphore_wait(barrier, 4 + has_below + has_above + has_across)
    halo = lambda where: remote(halo_out, halo_in, halo_sem.at[0], halo_sem.at[1], {"sp": where})

    @pl.when(me < count - 1)
    def _():
        halo(me + 1).start()

    convolve(halo_rows, tok_rows - halo_rows)

    @pl.when(me == 0)
    def _():
        padded_ref[:halo_rows, :] = jnp.zeros((halo_rows, gated.shape[1]), f32)

    @pl.when(me > 0)
    def _():
        halo(me).wait_recv()
        padded_ref[:halo_rows, :] = halo_in[...].astype(f32)

    convolve(0, halo_rows)

    conv_out = conv_ref[...]
    diagonal = lax.broadcasted_iota(jnp.int32, (tok_rows, tok_rows), 0) == lax.broadcasted_iota(
        jnp.int32, (tok_rows, tok_rows), 1
    )

    def lying(column):
        return jnp.sum(jnp.where(diagonal, column, 0.0), axis=0, keepdims=True)

    def standing(line):
        return jnp.sum(jnp.where(diagonal, line, 0.0), axis=1, keepdims=True)

    stat_out[0:1, :] = lying(jnp.sum(conv_out, axis=1, keepdims=True))
    stat_out[1:2, :] = lying(jnp.sum(conv_out * conv_out, axis=1, keepdims=True))
    stats = [
        remote(stat_out, stat_in.at[at], stat_send.at[at], stat_recv.at[at], peer)
        for at, peer in enumerate((core_peer, row_peer, far_peer))
    ]
    for copy in stats:
        copy.start()
    for load in loads[4:9]:
        load.wait()
    for copy in stats:
        copy.wait_recv()
    sums = (stat_out[...] + stat_in[0]) + (stat_in[1] + stat_in[2])
    channel_mean = standing(sums[0:1]) / channels_all
    channel_var = standing(sums[1:2]) / channels_all - channel_mean * channel_mean
    scaled = (conv_out - channel_mean) * lax.rsqrt(channel_var + LN_EPS) * ln_gain_ref[
        ...
    ] + ln_bias_ref[...]
    mixed = silu(scaled).astype(bf16)

    give_at = pl.ds(pl.multiple_of((1 - core) * half_width, half_width), half_width)
    give_out[...] = jnp.dot(mixed, w_out_ref[:, give_at], preferred_element_type=f32).astype(bf16)

    def cut(at):
        return pl.ds(at * cut_rows, cut_rows)

    gives = [
        remote(
            give_out.at[cut(at)], give_in.at[cut(at)], give_send.at[at], give_recv.at[at], core_peer
        )
        for at in range(ROW_CUTS)
    ]
    for copy in gives:
        copy.start()
    keep_ref[...] = jnp.dot(mixed, w_out_ref[:, half_at], preferred_element_type=f32)
    chips = [
        remote(
            chip_out.at[cut(at)], chip_in.at[cut(at)], chip_send.at[at], chip_recv.at[at], row_peer
        )
        for at in range(ROW_CUTS)
    ]
    for at in range(ROW_CUTS):
        gives[at].wait_recv()
        chip_sum = keep_ref[cut(at), :] + give_in[cut(at), :].astype(f32)
        keep_ref[cut(at), :] = chip_sum
        chip_out[cut(at), :] = chip_sum.astype(bf16)
        chips[at].start()

    def block(half, at, piece):
        return rows_ref.at[half, at, cut(piece)]

    def up_copy(origin, piece):
        at = origin * 2 + side
        sem = origin * ROW_CUTS + piece
        spot = block(core, at, piece)
        return remote(spot, spot, up_sem.at[sem], main_recv.at[at * ROW_CUTS + piece], {"sp": me + 2})

    def low_copy(origin, piece):
        at = origin * 2 + side
        sem = origin * ROW_CUTS + piece
        spot = block(core, at, piece)
        return remote(spot, spot, low_sem.at[sem], main_recv.at[at * ROW_CUTS + piece], {"sp": me - 2})

    def side_copy(origin, piece):
        at = origin * 2 + side
        sem = origin * ROW_CUTS + piece
        spot = block(core, at, piece)
        return remote(spot, spot, side_sem.at[sem], main_recv.at[at * ROW_CUTS + piece], side_peer)

    def core_copy(at, piece):
        sem = at * ROW_CUTS + piece
        spot = block(core, at, piece)
        return remote(spot, spot, core_sem.at[sem], core_recv.at[sem], core_peer)

    def landed(at, piece):
        spot = block(core, at, piece)
        sem = at * ROW_CUTS + piece
        remote(spot, spot, core_sem.at[sem], main_recv.at[sem], core_peer).wait_recv()

    def crossed(at, piece):
        spot = block(1 - core, at, piece)
        sem = at * ROW_CUTS + piece
        remote(spot, spot, core_sem.at[sem], core_recv.at[sem], core_peer).wait_recv()

    def settle(piece):
        chips[piece].wait_recv()
        total = keep_ref[cut(piece), :] + chip_in[cut(piece), :].astype(f32)
        rows_ref[core, me, cut(piece), :] = (resid_ref[cut(piece), :].astype(f32) + total).astype(bf16)
        core_copy(me, piece).start()
        side_copy(level, piece).start()

        @pl.when(level < levels - 1)
        def _():
            up_copy(level, piece).start()

        @pl.when(level > 0)
        def _():
            low_copy(level, piece).start()

    def normalise(at, some):
        low = rows_ref[0, at, some, :].astype(f32)
        high = rows_ref[1, at, some, :].astype(f32)
        power = jnp.sum(low * low, axis=1, keepdims=True) + jnp.sum(high * high, axis=1, keepdims=True)
        inverse = lax.rsqrt(power / model_width + RMS_EPS)
        normed_ref[some, :half_width] = (low * inverse * ffn_gain_ref[:, :half_width]).astype(bf16)
        normed_ref[some, half_width:] = (high * inverse * ffn_gain_ref[:, half_width:]).astype(bf16)

    def far_copy(at, piece):
        spot = hidden_ref.at[tp_place, at, cut(piece)]
        sem = at * ROW_CUTS + piece
        return remote(spot, spot, far_send.at[sem], far_recv.at[sem], row_peer)

    def near_copy(at, piece):
        spot = hidden_ref.at[tp_place, at, cut(piece)]
        sem = at * ROW_CUTS + piece
        return remote(spot, spot, near_send.at[sem], near_recv.at[sem], core_peer)

    def relay_copy(at, piece):
        spot = hidden_ref.at[row_place, at, cut(piece)]
        sem = at * ROW_CUTS + piece
        return remote(spot, spot, relay_send.at[sem], relay_recv.at[sem], core_peer)

    shared_far = remote(
        shared_ref.at[tp_place], shared_ref.at[tp_place], shared_send.at[0], shared_recv.at[0], row_peer
    )
    shared_near = remote(
        shared_ref.at[tp_place], shared_ref.at[tp_place], shared_send.at[1], shared_recv.at[1], core_peer
    )
    shared_relay = remote(
        shared_ref.at[row_place], shared_ref.at[row_place], shared_send.at[2], shared_recv.at[2], core_peer
    )

    every = range(ROW_CUTS)

    def hide(at, pieces):
        some = pl.ds(pieces[0] * cut_rows, len(pieces) * cut_rows)
        for piece in pieces:
            crossed(at, piece)
        normalise(at, some)
        hide_rows(at, pieces)

    def hide_rows(at, pieces):
        some = pl.ds(pieces[0] * cut_rows, len(pieces) * cut_rows)
        step = 256
        for first in range(0, part_hidden, step):
            wide = slice(first, first + step)
            gate_part = jnp.dot(normed_ref[some, :], gate_ref[:, wide], preferred_element_type=f32)
            up_part = jnp.dot(normed_ref[some, :], up_ref[:, wide], preferred_element_type=f32)
            hidden_ref[tp_place, at, some, wide] = (silu(gate_part) * up_part).astype(bf16)
        for piece in pieces:
            far_copy(at, piece).start()
        for piece in pieces:
            near_copy(at, piece).start()

    def down_part(at, some, place):
        return jnp.dot(
            hidden_ref[place, at, some, :],
            down_ref[pl.ds(pl.multiple_of(place * part_hidden, part_hidden), part_hidden), :],
            preferred_element_type=f32,
        )

    def back_copy(at):
        return remote(part_ref.at[at], back_ref.at[me], back_send.at[at], back_recv.at[me], {"sp": at})

    def relay(at, piece):
        far_copy(at, piece).wait_recv()
        relay_copy(at, piece).start()

    def finish(at):
        for piece in every:
            relay(at, piece)
        for piece in every:
            near_copy(at, piece).wait_recv()
        for piece in every:
            relay_copy(at, piece).wait_recv()
        some = pl.ds(0, tok_rows)
        total = (down_part(at, some, 0) + down_part(at, some, 1)) + (
            down_part(at, some, 2) + down_part(at, some, 3)
        )
        part_ref[at] = total.astype(bf16)
        back_copy(at).start()

    def pass_on(step, piece):
        below = level - step
        above = level + step

        @pl.when(below >= 0)
        def _():
            landed(below * 2 + side, piece)

            @pl.when(level < levels - 1)
            def _():
                up_copy(below, piece).start()

            side_copy(below, piece).start()
            core_copy(below * 2 + side, piece).start()

        @pl.when(above < levels)
        def _():
            landed(above * 2 + side, piece)

            @pl.when(level > 0)
            def _():
                low_copy(above, piece).start()

            side_copy(above, piece).start()
            core_copy(above * 2 + side, piece).start()

    def from_side(at):
        for piece in every:
            landed(at, piece)
            core_copy(at, piece).start()

    upper = (2 * level) // levels
    inner = level + upper * (levels - 1 - 2 * level)

    def visited(outer_way, inner_way):
        mirrored = outer_way[0] + inner * (inner_way[0] - outer_way[0])
        other = outer_way[1] + inner * (inner_way[1] - outer_way[1])
        at_level = mirrored + upper * (levels - 1 - 2 * mirrored)
        return at_level * 2 + lax.rem(side + other, 2), other

    outer_order = ((0, 1), (1, 0), (2, 0), (3, 0), (2, 1), (3, 1), (1, 1))
    inner_order = ((0, 0), (2, 0), (3, 0), (2, 1), (0, 1), (3, 1), (1, 1))
    visits = [visited(*ways) for ways in zip(outer_order, inner_order)]

    settle(0)
    for load in loads[9:13]:
        load.wait()
    hide(me, (0,))
    settle(1)
    first = visits[0][0]
    beside = level * 2 + (1 - side)
    for piece in every:
        landed(beside, piece)
        core_copy(beside, piece).start()
        pass_on(1, piece)
        hide(first, (piece,))
    for load in loads[13:]:
        load.wait()
    hide(visits[1][0], every)
    for piece in every:
        pass_on(2, piece)
    relay(me, 0)
    finish(first)

    crossed(me, 1)
    whole = pl.ds(0, tok_rows)
    normalise(me, whole)
    shared_gate = jnp.dot(normed_ref[...], sh_gate_ref[...], preferred_element_type=f32)
    shared_up = jnp.dot(normed_ref[...], sh_up_ref[...], preferred_element_type=f32)
    shared_ref[tp_place] = (silu(shared_gate) * shared_up).astype(bf16)

    for turn in range(2, len(visits)):
        at, other = visits[turn]
        hide(at, every)
        if turn == 2:
            for piece in every:
                pass_on(3, piece)
            shared_far.start()
            shared_near.start()
        if turn + 1 < len(visits):
            after, after_other = visits[turn + 1]

            @pl.when(after_other == 1)
            def _():
                @pl.when(after != beside)
                def _():
                    from_side(after)

        finish(visits[turn - 1][0])

    normalise(me, cut(1))
    hide_rows(me, (1,))
    finish(visits[-1][0])

    middle_cols = rows_ref[row, me, :, pl.ds(pl.multiple_of(core * col_width, col_width), col_width)]
    shared_far.wait_recv()
    shared_relay.start()
    shared_near.wait_recv()
    shared_relay.wait_recv()
    total = middle_cols.astype(f32)
    shared_width = shared_ref.shape[2]
    for place in range(4):
        total = total + jnp.dot(
            shared_ref[place],
            sh_down_ref[place * shared_width : (place + 1) * shared_width, :],
            preferred_element_type=f32,
        )
    sum_ref[...] = total

    for piece in every:
        near_copy(me, piece).wait_recv()
    relay_copy(me, 0).wait_recv()
    own_part = down_part(me, whole, tp_place) + down_part(me, whole, core_place)
    relay(me, 1)
    own_part = own_part + down_part(me, whole, row_place)
    relay_copy(me, 1).wait_recv()
    own_part = own_part + down_part(me, whole, (1 - row) * 2 + (1 - core))
    part_ref[me] = own_part.astype(bf16)
    total = sum_ref[...]
    routes = routes_ref[...]
    route_weights = route_weights_ref[...]
    own_weight = standing(jnp.sum(jnp.where(routes == me, route_weights, 0.0), axis=0, keepdims=True))
    total = total + own_weight * part_ref[me].astype(f32)
    for step in range(1, count):
        at = lax.rem(me + step, count)
        remote(
            part_ref.at[at], back_ref.at[at], back_send.at[at], back_recv.at[at], core_peer
        ).wait_recv()
        weight = standing(jnp.sum(jnp.where(routes == at, route_weights, 0.0), axis=0, keepdims=True))
        total = total + weight * back_ref[at].astype(f32)
    out_ref[...] = total.astype(bf16)

    @pl.when(me < count - 1)
    def _():
        halo(me + 1).wait_send()

    for copy in stats + gives + chips + [shared_far, shared_near, shared_relay]:
        copy.wait_send()

    @pl.loop(0, levels)
    def _(origin):
        for piece in range(ROW_CUTS):
            side_copy(origin, piece).wait_send()

            @pl.when((level < levels - 1) & (origin <= level))
            def _():
                up_copy(origin, piece).wait_send()

            @pl.when((level > 0) & (origin >= level))
            def _():
                low_copy(origin, piece).wait_send()

    @pl.loop(0, count)
    def _(at):
        for piece in every:
            core_copy(at, piece).wait_send()
            far_copy(at, piece).wait_send()
            near_copy(at, piece).wait_send()
            relay_copy(at, piece).wait_send()

        @pl.when(at != me)
        def _():
            back_copy(at).wait_send()


def body_dense(
    resid,
    a_val,
    a_gate,
    conv_kernel,
    conv_bias,
    ln_gain,
    ln_bias,
    w_out,
    ffn_gain,
    routes,
    route_weights,
    exp_gate,
    exp_up,
    exp_down,
    sh_gate,
    sh_up,
    sh_down,
):
    count = lax.axis_size("sp")
    levels = count // 2
    tok_rows, model_width = resid.shape
    half_width = model_width // 2
    channels = a_val.shape[1]
    part_hidden = exp_gate.shape[2]
    col_width = exp_down.shape[2]
    shared_width = sh_gate.shape[1]
    top_count = routes.shape[1]
    span = conv_kernel.shape[0]
    halo_rows = -(-(span - 1) // 16) * 16
    vmem = pl.BlockSpec(memory_space=pltpu.VMEM)
    hbm = pl.BlockSpec(memory_space=pltpu.HBM)
    f32, bf16 = jnp.float32, jnp.bfloat16
    dma = pltpu.SemaphoreType.DMA
    operands = (
        resid,
        a_val,
        a_gate,
        conv_kernel,
        conv_bias.reshape(1, -1),
        ln_gain.reshape(1, -1),
        ln_bias.reshape(1, -1),
        w_out,
        ffn_gain.reshape(1, -1),
        routes.T,
        route_weights.T,
        exp_gate[0],
        exp_up[0],
        exp_down[0],
        sh_gate,
        sh_up,
        sh_down,
    )
    pieces = count * ROW_CUTS
    return pl.pallas_call(
        functools.partial(layer_kernel, levels),
        out_shape=jax.ShapeDtypeStruct((tok_rows, col_width), bf16),
        in_specs=[hbm] * len(operands),
        out_specs=vmem,
        scratch_shapes=[
            pltpu.VMEM((tok_rows, half_width), bf16),
            pltpu.VMEM(a_val.shape, bf16),
            pltpu.VMEM(a_gate.shape, bf16),
            pltpu.VMEM(conv_kernel.shape, bf16),
            pltpu.VMEM((1, channels), f32),
            pltpu.VMEM((1, channels), f32),
            pltpu.VMEM((1, channels), f32),
            pltpu.VMEM(w_out.shape, bf16),
            pltpu.VMEM((1, model_width), f32),
            pltpu.VMEM((top_count, tok_rows), jnp.int32),
            pltpu.VMEM((top_count, tok_rows), f32),
            pltpu.VMEM(exp_gate.shape[1:], bf16),
            pltpu.VMEM(exp_up.shape[1:], bf16),
            pltpu.VMEM(exp_down.shape[1:], bf16),
            pltpu.VMEM(sh_gate.shape, bf16),
            pltpu.VMEM(sh_up.shape, bf16),
            pltpu.VMEM(sh_down.shape, bf16),
            pltpu.VMEM((halo_rows, channels), bf16),
            pltpu.VMEM((halo_rows, channels), bf16),
            pltpu.VMEM((halo_rows + tok_rows, channels), f32),
            pltpu.VMEM((tok_rows, channels), f32),
            pltpu.VMEM((2, tok_rows), f32),
            pltpu.VMEM((3, 2, tok_rows), f32),
            pltpu.VMEM((tok_rows, half_width), bf16),
            pltpu.VMEM((tok_rows, half_width), bf16),
            pltpu.VMEM((tok_rows, half_width), f32),
            pltpu.VMEM((tok_rows, half_width), bf16),
            pltpu.VMEM((tok_rows, half_width), bf16),
            pltpu.VMEM((2, count, tok_rows, half_width), bf16),
            pltpu.VMEM((tok_rows, model_width), bf16),
            pltpu.VMEM((4, count, tok_rows, part_hidden), bf16),
            pltpu.VMEM((4, tok_rows, shared_width), bf16),
            pltpu.VMEM((count, tok_rows, col_width), bf16),
            pltpu.VMEM((count, tok_rows, col_width), bf16),
            pltpu.VMEM((tok_rows, col_width), f32),
            dma((17,)),
            dma((2,)),
            dma((3,)),
            dma((3,)),
            dma((ROW_CUTS,)),
            dma((ROW_CUTS,)),
            dma((ROW_CUTS,)),
            dma((ROW_CUTS,)),
            dma((levels * ROW_CUTS,)),
            dma((levels * ROW_CUTS,)),
            dma((levels * ROW_CUTS,)),
            dma((pieces,)),
            dma((pieces,)),
            dma((pieces,)),
            dma((pieces,)),
            dma((pieces,)),
            dma((pieces,)),
            dma((pieces,)),
            dma((pieces,)),
            dma((pieces,)),
            dma((3,)),
            dma((3,)),
            dma((count,)),
            dma((count,)),
        ],
        compiler_params=pltpu.CompilerParams(
            collective_id=0, has_side_effects=True, vmem_limit_bytes=56 * 1024 * 1024
        ),
    )(*operands)


def body(*args):
    tok_rows = args[0].shape[0]
    top_count = args[9].shape[1]
    local_experts = args[11].shape[0]
    experts_all = local_experts * lax.axis_size("sp")
    capacity = 2 * tok_rows * top_count // experts_all
    if (
        local_experts == 1
        and lax.axis_size("tp") == 4
        and lax.axis_size("sp") == 8
        and capacity >= tok_rows
    ):
        return body_dense(*args)
    return body_slots(*args)


def solution(mesh):
    in_specs = (
        P("sp", None),
        P("sp", "tp"),
        P("sp", "tp"),
        P(None, "tp"),
        P("tp"),
        P("tp"),
        P("tp"),
        P("tp", None),
        P(),
        P("sp", None),
        P("sp", None),
        P("sp", None, "tp"),
        P("sp", None, "tp"),
        P("sp", None, "tp"),
        P(None, "tp"),
        P(None, "tp"),
        P(None, "tp"),
    )
    out_specs = P("sp", "tp")
    return jax.shard_map(body, mesh=mesh, in_specs=in_specs, out_specs=out_specs, check_vma=False)
```

```python
import functools

import jax
import jax.numpy as jnp
from jax import lax
from jax.experimental import pallas as pl
from jax.experimental.pallas import tpu as pltpu
from jax.sharding import PartitionSpec as P

LN_EPS = 1e-05
RMS_EPS = 1e-06


def shifted(value, axis, by):
    size = lax.axis_size(axis)
    pairs = [(i, i + by) for i in range(size) if 0 <= i + by < size]
    return lax.ppermute(value, axis, pairs)


def body_slots(
    resid,
    a_val,
    a_gate,
    conv_kernel,
    conv_bias,
    ln_gain,
    ln_bias,
    w_out,
    ffn_gain,
    routes,
    route_weights,
    exp_gate,
    exp_up,
    exp_down,
    sh_gate,
    sh_up,
    sh_down,
):
    tp_count = lax.axis_size("tp")
    tp_place = lax.axis_index("tp")
    sp_count = lax.axis_size("sp")
    tok_rows = resid.shape[0]
    model_width = resid.shape[1]
    col_width = model_width // tp_count
    col_start = tp_place * col_width
    conv_span = conv_kernel.shape[0]
    channels_all = a_val.shape[1] * tp_count
    gated_in = (a_val.astype(jnp.float32) * jax.nn.sigmoid(a_gate.astype(jnp.float32))).astype(
        jnp.bfloat16
    )
    before = shifted(gated_in[tok_rows - (conv_span - 1) :], "sp", 1)
    padded = jnp.concatenate([before, gated_in], axis=0).astype(jnp.float32)
    kernel = conv_kernel.astype(jnp.float32)

    def add_tap(offset, running):
        window_rows = lax.dynamic_slice_in_dim(padded, offset, tok_rows, 0)
        return running + lax.dynamic_slice_in_dim(kernel, offset, 1, 0) * window_rows

    start_sum = jnp.broadcast_to(conv_bias[None, :], gated_in.shape)
    conv_out = lax.fori_loop(0, conv_span, add_tap, start_sum)
    row_sums = lax.psum((jnp.sum(conv_out, axis=1), jnp.sum(conv_out * conv_out, axis=1)), "tp")
    channel_mean = row_sums[0] / channels_all
    channel_var = row_sums[1] / channels_all - channel_mean * channel_mean
    scaled = (conv_out - channel_mean[:, None]) * lax.rsqrt(
        channel_var[:, None] + LN_EPS
    ) * ln_gain[None, :] + ln_bias[None, :]
    mixed_out = jax.nn.silu(scaled).astype(jnp.bfloat16)
    partial_proj = jnp.dot(mixed_out, w_out, preferred_element_type=jnp.float32)
    projected = lax.psum(partial_proj, "tp")
    middle = (resid.astype(jnp.float32) + projected).astype(jnp.bfloat16)
    middle_f = middle.astype(jnp.float32)
    inverse = lax.rsqrt(jnp.mean(middle_f * middle_f, axis=1, keepdims=True) + RMS_EPS)
    normed = (middle_f * inverse * ffn_gain[None, :]).astype(jnp.bfloat16)
    middle_cols = lax.dynamic_slice_in_dim(middle, col_start, col_width, 1)
    shared_gate = jnp.dot(normed, sh_gate, preferred_element_type=jnp.float32)
    shared_up = jnp.dot(normed, sh_up, preferred_element_type=jnp.float32)
    shared_hidden = (jax.nn.silu(shared_gate) * shared_up).astype(jnp.bfloat16)
    weight_rows = sh_down
    shared = jnp.dot(
        lax.all_gather(shared_hidden, "tp", axis=1, tiled=True),
        weight_rows,
        preferred_element_type=jnp.float32,
    )
    top_count = routes.shape[1]
    local_experts = exp_gate.shape[0]
    experts_all = local_experts * sp_count
    capacity = max(2 * tok_rows * top_count // experts_all, tp_count)
    pair_count = tok_rows * top_count
    chosen = routes.reshape(pair_count)
    one_hot = (chosen[:, None] == jnp.arange(experts_all, dtype=jnp.int32)[None, :]).astype(
        jnp.int32
    )
    earlier = jnp.cumsum(one_hot, axis=0) - one_hot
    place_in = jnp.sum(earlier * one_hot, axis=1)
    slot_of = chosen * capacity + place_in
    owner_ids = (
        jnp.zeros((experts_all * capacity,), jnp.int32)
        .at[slot_of]
        .set(jnp.arange(pair_count, dtype=jnp.int32) + 1)
    )
    owner_grid = owner_ids.reshape(sp_count, local_experts, capacity)
    part_slots = capacity // tp_count
    own_owners = lax.dynamic_slice_in_dim(owner_grid, tp_place * part_slots, part_slots, 2)
    source_row = jnp.maximum(own_owners - 1, 0) // top_count
    taken = normed[source_row.reshape(-1)].reshape(own_owners.shape + (model_width,))
    landed = lax.all_to_all(
        jnp.where((own_owners > 0)[..., None], taken, jnp.zeros((), jnp.bfloat16)),
        "sp",
        split_axis=0,
        concat_axis=0,
        tiled=True,
    )
    arrived = lax.all_gather(landed, "tp", axis=2, tiled=True)
    gate_part = jnp.einsum("sxcd,xdf->sxcf", arrived, exp_gate, preferred_element_type=jnp.float32)
    up_part = jnp.einsum("sxcd,xdf->sxcf", arrived, exp_up, preferred_element_type=jnp.float32)
    expert_hidden = (jax.nn.silu(gate_part) * up_part).astype(jnp.bfloat16)
    weight_rows = exp_down
    expert_sum = jnp.einsum(
        "sxcf,xfd->sxcd",
        lax.all_gather(expert_hidden, "tp", axis=3, tiled=True),
        weight_rows,
        preferred_element_type=jnp.float32,
    )
    expert_out = expert_sum.astype(jnp.bfloat16)
    returned = lax.all_to_all(expert_out, "sp", split_axis=0, concat_axis=0, tiled=True)
    flat_out = returned.reshape(experts_all * capacity, col_width)
    picked = flat_out[slot_of].astype(jnp.float32).reshape(tok_rows, top_count, col_width)
    routed = jnp.sum(picked * route_weights[:, :, None], axis=1)
    return (middle_cols.astype(jnp.float32) + shared + routed).astype(jnp.bfloat16)


ROW_CUTS = 2


def silu(value):
    return value / (1.0 + jnp.exp(-value))


def layer_kernel(
    levels,
    resid_hbm,
    a_val_hbm,
    a_gate_hbm,
    taps_hbm,
    conv_bias_hbm,
    ln_gain_hbm,
    ln_bias_hbm,
    w_out_hbm,
    ffn_gain_hbm,
    routes_hbm,
    route_weights_hbm,
    exp_gate_hbm,
    exp_up_hbm,
    exp_down_hbm,
    sh_gate_hbm,
    sh_up_hbm,
    sh_down_hbm,
    out_ref,
    resid_ref,
    a_val_ref,
    a_gate_ref,
    taps_ref,
    conv_bias_ref,
    ln_gain_ref,
    ln_bias_ref,
    w_out_ref,
    ffn_gain_ref,
    routes_ref,
    route_weights_ref,
    gate_ref,
    up_ref,
    down_ref,
    sh_gate_ref,
    sh_up_ref,
    sh_down_ref,
    halo_out,
    halo_in,
    padded_ref,
    conv_ref,
    stat_out,
    stat_in,
    mix_out,
    mix_in,
    w_in,
    keep_ref,
    chip_out,
    chip_in,
    rows_ref,
    normed_ref,
    hidden_ref,
    shared_ref,
    part_ref,
    back_ref,
    sum_ref,
    load_sem,
    halo_sem,
    stat_send,
    stat_recv,
    mix_sem,
    chip_send,
    chip_recv,
    up_sem,
    low_sem,
    side_sem,
    core_sem,
    main_recv,
    core_recv,
    far_send,
    far_recv,
    near_send,
    near_recv,
    relay_send,
    relay_recv,
    shared_send,
    shared_recv,
    back_send,
    back_recv,
):
    count = 2 * levels
    me = lax.axis_index("sp")
    tp_place = lax.axis_index("tp")
    level, side = me // 2, me % 2
    row, core = tp_place // 2, tp_place % 2
    core_place = row * 2 + (1 - core)
    row_place = (1 - row) * 2 + core
    core_peer = {"tp": core_place}
    row_peer = {"tp": row_place}
    far_peer = {"tp": (1 - row) * 2 + (1 - core)}
    side_peer = {"sp": level * 2 + (1 - side)}
    mesh_ids = pl.DeviceIdType.MESH
    f32, bf16 = jnp.float32, jnp.bfloat16
    tok_rows, half_width = resid_ref.shape
    model_width = 2 * half_width
    col_width = out_ref.shape[1]
    span = taps_ref.shape[0]
    halo_rows = halo_in.shape[0]
    channels_all = 4 * a_val_ref.shape[1]
    part_hidden = gate_ref.shape[1]
    cut_rows = tok_rows // ROW_CUTS

    half_at = pl.ds(pl.multiple_of(core * half_width, half_width), half_width)
    pairs = [
        (a_val_hbm, a_val_ref),
        (a_gate_hbm, a_gate_ref),
        (taps_hbm, taps_ref),
        (conv_bias_hbm, conv_bias_ref),
        (ln_gain_hbm, ln_gain_ref),
        (ln_bias_hbm, ln_bias_ref),
        (w_out_hbm.at[:, half_at], w_out_ref),
        (resid_hbm.at[:, half_at], resid_ref),
        (ffn_gain_hbm, ffn_gain_ref),
        (exp_gate_hbm, gate_ref),
        (exp_up_hbm, up_ref),
        (sh_gate_hbm, sh_gate_ref),
        (sh_up_hbm, sh_up_ref),
        (exp_down_hbm, down_ref),
        (sh_down_hbm, sh_down_ref),
        (routes_hbm, routes_ref),
        (route_weights_hbm, route_weights_ref),
    ]
    loads = [
        pltpu.make_async_copy(src, dst, load_sem.at[at]) for at, (src, dst) in enumerate(pairs)
    ]
    for load in loads:
        load.start()

    barrier = pltpu.get_barrier_semaphore()

    def greet(peer):
        pl.semaphore_signal(barrier, inc=1, device_id=peer, device_id_type=mesh_ids)

    across = ((side == 0) & (level > 0)) | ((side == 1) & (level < levels - 1))
    for peer in (core_peer, row_peer, far_peer, side_peer):
        greet(peer)

    @pl.when(level > 0)
    def _():
        greet({"sp": me - 2})

    @pl.when(level < levels - 1)
    def _():
        greet({"sp": me + 2})

    @pl.when(across)
    def _():
        greet({"sp": me + 2 * side - 1})

    def remote(src, dst, send, recv, where):
        return pltpu.make_async_remote_copy(
            src_ref=src, dst_ref=dst, send_sem=send, recv_sem=recv, device_id=where, device_id_type=mesh_ids
        )

    for load in loads[:4]:
        load.wait()
    gated = (a_val_ref[...].astype(f32) / (1.0 + jnp.exp(-a_gate_ref[...].astype(f32)))).astype(bf16)
    halo_out[...] = gated[tok_rows - halo_rows :]
    padded_ref[halo_rows:, :] = gated.astype(f32)
    taps = taps_ref[...].astype(f32)

    def convolve(first, size):
        total = jnp.broadcast_to(conv_bias_ref[...], (size, gated.shape[1]))
        for tap in range(span):
            at = first + tap + halo_rows - (span - 1)
            total = total + taps[tap : tap + 1] * padded_ref[at : at + size, :]
        conv_ref[first : first + size, :] = total

    has_below = (level + levels - 2) // (levels - 1)
    has_above = (2 * levels - 3 - level) // (levels - 1)
    has_across = has_below + side * (has_above - has_below)
    pl.semaphore_wait(barrier, 4 + has_below + has_above + has_across)
    give_at = pl.ds(pl.multiple_of((1 - core) * half_width, half_width), half_width)
    w_swap = remote(w_out_hbm.at[:, give_at], w_in, mix_sem.at[2], mix_sem.at[3], core_peer)
    halo = lambda where: remote(halo_out, halo_in, halo_sem.at[0], halo_sem.at[1], {"sp": where})

    @pl.when(me < count - 1)
    def _():
        halo(me + 1).start()

    w_swap.start()
    convolve(halo_rows, tok_rows - halo_rows)

    @pl.when(me == 0)
    def _():
        padded_ref[:halo_rows, :] = jnp.zeros((halo_rows, gated.shape[1]), f32)

    @pl.when(me > 0)
    def _():
        halo(me).wait_recv()
        padded_ref[:halo_rows, :] = halo_in[...].astype(f32)

    convolve(0, halo_rows)

    conv_out = conv_ref[...]
    diagonal = lax.broadcasted_iota(jnp.int32, (tok_rows, tok_rows), 0) == lax.broadcasted_iota(
        jnp.int32, (tok_rows, tok_rows), 1
    )

    def lying(column):
        return jnp.sum(jnp.where(diagonal, column, 0.0), axis=0, keepdims=True)

    def standing(line):
        return jnp.sum(jnp.where(diagonal, line, 0.0), axis=1, keepdims=True)

    stat_out[0:1, :] = lying(jnp.sum(conv_out, axis=1, keepdims=True))
    stat_out[1:2, :] = lying(jnp.sum(conv_out * conv_out, axis=1, keepdims=True))
    stats = [
        remote(stat_out, stat_in.at[at], stat_send.at[at], stat_recv.at[at], peer)
        for at, peer in enumerate((core_peer, row_peer, far_peer))
    ]
    for copy in stats:
        copy.start()
    for load in loads[4:9]:
        load.wait()
    for copy in stats:
        copy.wait_recv()
    sums = (stat_out[...] + stat_in[0]) + (stat_in[1] + stat_in[2])
    channel_mean = standing(sums[0:1]) / channels_all
    channel_var = standing(sums[1:2]) / channels_all - channel_mean * channel_mean
    scaled = (conv_out - channel_mean) * lax.rsqrt(channel_var + LN_EPS) * ln_gain_ref[
        ...
    ] + ln_bias_ref[...]
    mix_out[...] = silu(scaled).astype(bf16)

    def cut(at):
        return pl.ds(at * cut_rows, cut_rows)

    mix = remote(mix_out, mix_in, mix_sem.at[0], mix_sem.at[1], core_peer)
    mix.start()
    keep_ref[...] = jnp.dot(mix_out[...], w_out_ref[...], preferred_element_type=f32)
    w_swap.wait_recv()
    chips = [
        remote(
            chip_out.at[cut(at)], chip_in.at[cut(at)], chip_send.at[at], chip_recv.at[at], row_peer
        )
        for at in range(ROW_CUTS)
    ]
    mix.wait_recv()
    for at in range(ROW_CUTS):
        chip_sum = keep_ref[cut(at), :] + jnp.dot(
            mix_in[cut(at), :], w_in[...], preferred_element_type=f32
        )
        keep_ref[cut(at), :] = chip_sum
        chip_out[cut(at), :] = chip_sum.astype(bf16)
        chips[at].start()

    def block(half, at, piece):
        return rows_ref.at[half, at, cut(piece)]

    def up_copy(origin, piece):
        at = origin * 2 + side
        sem = origin * ROW_CUTS + piece
        spot = block(core, at, piece)
        return remote(spot, spot, up_sem.at[sem], main_recv.at[at * ROW_CUTS + piece], {"sp": me + 2})

    def low_copy(origin, piece):
        at = origin * 2 + side
        sem = origin * ROW_CUTS + piece
        spot = block(core, at, piece)
        return remote(spot, spot, low_sem.at[sem], main_recv.at[at * ROW_CUTS + piece], {"sp": me - 2})

    def side_copy(origin, piece):
        at = origin * 2 + side
        sem = origin * ROW_CUTS + piece
        spot = block(core, at, piece)
        return remote(spot, spot, side_sem.at[sem], main_recv.at[at * ROW_CUTS + piece], side_peer)

    def core_copy(at, piece):
        sem = at * ROW_CUTS + piece
        spot = block(core, at, piece)
        return remote(spot, spot, core_sem.at[sem], core_recv.at[sem], core_peer)

    def landed(at, piece):
        spot = block(core, at, piece)
        sem = at * ROW_CUTS + piece
        remote(spot, spot, core_sem.at[sem], main_recv.at[sem], core_peer).wait_recv()

    def crossed(at, piece):
        spot = block(1 - core, at, piece)
        sem = at * ROW_CUTS + piece
        remote(spot, spot, core_sem.at[sem], core_recv.at[sem], core_peer).wait_recv()

    def settle(piece):
        chips[piece].wait_recv()
        total = keep_ref[cut(piece), :] + chip_in[cut(piece), :].astype(f32)
        rows_ref[core, me, cut(piece), :] = (resid_ref[cut(piece), :].astype(f32) + total).astype(bf16)
        core_copy(me, piece).start()
        side_copy(level, piece).start()

        @pl.when(level < levels - 1)
        def _():
            up_copy(level, piece).start()

        @pl.when(level > 0)
        def _():
            low_copy(level, piece).start()

    def normalise(at, some):
        low = rows_ref[0, at, some, :].astype(f32)
        high = rows_ref[1, at, some, :].astype(f32)
        power = jnp.sum(low * low, axis=1, keepdims=True) + jnp.sum(high * high, axis=1, keepdims=True)
        inverse = lax.rsqrt(power / model_width + RMS_EPS)
        normed_ref[some, :half_width] = (low * inverse * ffn_gain_ref[:, :half_width]).astype(bf16)
        normed_ref[some, half_width:] = (high * inverse * ffn_gain_ref[:, half_width:]).astype(bf16)

    def far_copy(at, piece):
        spot = hidden_ref.at[tp_place, at, cut(piece)]
        sem = at * ROW_CUTS + piece
        return remote(spot, spot, far_send.at[sem], far_recv.at[sem], row_peer)

    def near_copy(at, piece):
        spot = hidden_ref.at[tp_place, at, cut(piece)]
        sem = at * ROW_CUTS + piece
        return remote(spot, spot, near_send.at[sem], near_recv.at[sem], core_peer)

    def relay_copy(at, piece):
        spot = hidden_ref.at[row_place, at, cut(piece)]
        sem = at * ROW_CUTS + piece
        return remote(spot, spot, relay_send.at[sem], relay_recv.at[sem], core_peer)

    shared_far = remote(
        shared_ref.at[tp_place], shared_ref.at[tp_place], shared_send.at[0], shared_recv.at[0], row_peer
    )
    shared_near = remote(
        shared_ref.at[tp_place], shared_ref.at[tp_place], shared_send.at[1], shared_recv.at[1], core_peer
    )
    shared_relay = remote(
        shared_ref.at[row_place], shared_ref.at[row_place], shared_send.at[2], shared_recv.at[2], core_peer
    )

    every = range(ROW_CUTS)

    def hide(at, pieces):
        some = pl.ds(pieces[0] * cut_rows, len(pieces) * cut_rows)
        for piece in pieces:
            crossed(at, piece)
        normalise(at, some)
        hide_rows(at, pieces)

    def hide_rows(at, pieces):
        some = pl.ds(pieces[0] * cut_rows, len(pieces) * cut_rows)
        step = 256
        for first in range(0, part_hidden, step):
            wide = slice(first, first + step)
            gate_part = jnp.dot(normed_ref[some, :], gate_ref[:, wide], preferred_element_type=f32)
            up_part = jnp.dot(normed_ref[some, :], up_ref[:, wide], preferred_element_type=f32)
            hidden_ref[tp_place, at, some, wide] = (silu(gate_part) * up_part).astype(bf16)
        for piece in pieces:
            far_copy(at, piece).start()
        for piece in pieces:
            near_copy(at, piece).start()

    def down_part(at, some, place):
        return jnp.dot(
            hidden_ref[place, at, some, :],
            down_ref[pl.ds(pl.multiple_of(place * part_hidden, part_hidden), part_hidden), :],
            preferred_element_type=f32,
        )

    def back_copy(at, piece):
        return remote(
            part_ref.at[at, cut(piece)],
            back_ref.at[me, cut(piece)],
            back_send.at[at * ROW_CUTS + piece],
            back_recv.at[me * ROW_CUTS + piece],
            {"sp": at},
        )

    def relay(at, piece):
        far_copy(at, piece).wait_recv()
        relay_copy(at, piece).start()

    def finish(at, pieces):
        for piece in pieces:
            relay(at, piece)
        for piece in pieces:
            near_copy(at, piece).wait_recv()
        for piece in pieces:
            relay_copy(at, piece).wait_recv()
        some = pl.ds(pieces[0] * cut_rows, len(pieces) * cut_rows)
        total = (down_part(at, some, 0) + down_part(at, some, 1)) + (
            down_part(at, some, 2) + down_part(at, some, 3)
        )
        part_ref[at, some, :] = total.astype(bf16)
        for piece in pieces:
            back_copy(at, piece).start()

    def pass_on(step, piece):
        below = level - step
        above = level + step

        @pl.when(below >= 0)
        def _():
            landed(below * 2 + side, piece)

            @pl.when(level < levels - 1)
            def _():
                up_copy(below, piece).start()

            side_copy(below, piece).start()
            core_copy(below * 2 + side, piece).start()

        @pl.when(above < levels)
        def _():
            landed(above * 2 + side, piece)

            @pl.when(level > 0)
            def _():
                low_copy(above, piece).start()

            side_copy(above, piece).start()
            core_copy(above * 2 + side, piece).start()

    def from_side(at):
        for piece in every:
            landed(at, piece)
            core_copy(at, piece).start()

    upper = (2 * level) // levels
    inner = level + upper * (levels - 1 - 2 * level)

    def visited(outer_way, inner_way):
        mirrored = outer_way[0] + inner * (inner_way[0] - outer_way[0])
        other = outer_way[1] + inner * (inner_way[1] - outer_way[1])
        at_level = mirrored + upper * (levels - 1 - 2 * mirrored)
        return at_level * 2 + lax.rem(side + other, 2), other

    outer_order = ((0, 1), (1, 0), (2, 0), (3, 0), (2, 1), (3, 1), (1, 1))
    inner_order = ((0, 0), (2, 0), (3, 0), (2, 1), (0, 1), (3, 1), (1, 1))
    visits = [visited(*ways) for ways in zip(outer_order, inner_order)]

    settle(0)
    for load in loads[9:13]:
        load.wait()
    hide(me, (0,))
    settle(1)
    first = visits[0][0]
    beside = level * 2 + (1 - side)
    for piece in every:
        landed(beside, piece)
        core_copy(beside, piece).start()
        pass_on(1, piece)
        hide(first, (piece,))
    for load in loads[13:]:
        load.wait()
    hide(visits[1][0], every)
    for piece in every:
        pass_on(2, piece)
    relay(me, 0)
    whole = pl.ds(0, tok_rows)

    def fetch(turn):
        at, other = visits[turn]

        @pl.when(other == 1)
        def _():
            @pl.when(at != beside)
            def _():
                from_side(at)

    for turn in range(2, len(visits)):
        at = visits[turn][0]
        hide(at, every)
        if turn + 1 < len(visits):
            fetch(turn + 1)
        finish(visits[turn - 2][0], every)
        if turn == 2:
            for piece in every:
                pass_on(3, piece)
        if turn == 4:
            crossed(me, 1)
            normalise(me, whole)
            shared_gate = jnp.dot(normed_ref[...], sh_gate_ref[...], preferred_element_type=f32)
            shared_up = jnp.dot(normed_ref[...], sh_up_ref[...], preferred_element_type=f32)
            shared_ref[tp_place] = (silu(shared_gate) * shared_up).astype(bf16)
            shared_far.start()
            shared_near.start()

    normalise(me, cut(1))
    hide_rows(me, (1,))
    middle_cols = rows_ref[row, me, :, pl.ds(pl.multiple_of(core * col_width, col_width), col_width)]
    shared_far.wait_recv()
    shared_relay.start()
    shared_near.wait_recv()
    shared_relay.wait_recv()
    total = middle_cols.astype(f32)
    shared_width = shared_ref.shape[2]
    for place in range(4):
        total = total + jnp.dot(
            shared_ref[place],
            sh_down_ref[place * shared_width : (place + 1) * shared_width, :],
            preferred_element_type=f32,
        )
    sum_ref[...] = total
    finish(visits[-2][0], every)
    for piece in every:
        finish(visits[-1][0], (piece,))

    for piece in every:
        near_copy(me, piece).wait_recv()
    relay_copy(me, 0).wait_recv()
    own_part = down_part(me, whole, tp_place) + down_part(me, whole, core_place)
    relay(me, 1)
    own_part = own_part + down_part(me, whole, row_place)
    relay_copy(me, 1).wait_recv()
    own_part = own_part + down_part(me, whole, (1 - row) * 2 + (1 - core))
    part_ref[me] = own_part.astype(bf16)
    total = sum_ref[...]
    routes = routes_ref[...]
    route_weights = route_weights_ref[...]
    own_weight = standing(jnp.sum(jnp.where(routes == me, route_weights, 0.0), axis=0, keepdims=True))
    total = total + own_weight * part_ref[me].astype(f32)
    for step in range(1, count):
        at = lax.rem(me + step, count)
        for piece in every:
            remote(
                part_ref.at[at, cut(piece)],
                back_ref.at[at, cut(piece)],
                back_send.at[at * ROW_CUTS + piece],
                back_recv.at[at * ROW_CUTS + piece],
                core_peer,
            ).wait_recv()
        weight = standing(jnp.sum(jnp.where(routes == at, route_weights, 0.0), axis=0, keepdims=True))
        total = total + weight * back_ref[at].astype(f32)
    out_ref[...] = total.astype(bf16)

    @pl.when(me < count - 1)
    def _():
        halo(me + 1).wait_send()

    for copy in stats + chips + [w_swap, mix, shared_far, shared_near, shared_relay]:
        copy.wait_send()

    @pl.loop(0, levels)
    def _(origin):
        for piece in range(ROW_CUTS):
            side_copy(origin, piece).wait_send()

            @pl.when((level < levels - 1) & (origin <= level))
            def _():
                up_copy(origin, piece).wait_send()

            @pl.when((level > 0) & (origin >= level))
            def _():
                low_copy(origin, piece).wait_send()

    @pl.loop(0, count)
    def _(at):
        for piece in every:
            core_copy(at, piece).wait_send()
            far_copy(at, piece).wait_send()
            near_copy(at, piece).wait_send()
            relay_copy(at, piece).wait_send()

        @pl.when(at != me)
        def _():
            for piece in every:
                back_copy(at, piece).wait_send()


def body_dense(
    resid,
    a_val,
    a_gate,
    conv_kernel,
    conv_bias,
    ln_gain,
    ln_bias,
    w_out,
    ffn_gain,
    routes,
    route_weights,
    exp_gate,
    exp_up,
    exp_down,
    sh_gate,
    sh_up,
    sh_down,
):
    count = lax.axis_size("sp")
    levels = count // 2
    tok_rows, model_width = resid.shape
    half_width = model_width // 2
    channels = a_val.shape[1]
    part_hidden = exp_gate.shape[2]
    col_width = exp_down.shape[2]
    shared_width = sh_gate.shape[1]
    top_count = routes.shape[1]
    span = conv_kernel.shape[0]
    halo_rows = -(-(span - 1) // 16) * 16
    vmem = pl.BlockSpec(memory_space=pltpu.VMEM)
    hbm = pl.BlockSpec(memory_space=pltpu.HBM)
    f32, bf16 = jnp.float32, jnp.bfloat16
    dma = pltpu.SemaphoreType.DMA
    operands = (
        resid,
        a_val,
        a_gate,
        conv_kernel,
        conv_bias.reshape(1, -1),
        ln_gain.reshape(1, -1),
        ln_bias.reshape(1, -1),
        w_out,
        ffn_gain.reshape(1, -1),
        routes.T,
        route_weights.T,
        exp_gate[0],
        exp_up[0],
        exp_down[0],
        sh_gate,
        sh_up,
        sh_down,
    )
    pieces = count * ROW_CUTS
    return pl.pallas_call(
        functools.partial(layer_kernel, levels),
        out_shape=jax.ShapeDtypeStruct((tok_rows, col_width), bf16),
        in_specs=[hbm] * len(operands),
        out_specs=vmem,
        scratch_shapes=[
            pltpu.VMEM((tok_rows, half_width), bf16),
            pltpu.VMEM(a_val.shape, bf16),
            pltpu.VMEM(a_gate.shape, bf16),
            pltpu.VMEM(conv_kernel.shape, bf16),
            pltpu.VMEM((1, channels), f32),
            pltpu.VMEM((1, channels), f32),
            pltpu.VMEM((1, channels), f32),
            pltpu.VMEM((channels, half_width), bf16),
            pltpu.VMEM((1, model_width), f32),
            pltpu.VMEM((top_count, tok_rows), jnp.int32),
            pltpu.VMEM((top_count, tok_rows), f32),
            pltpu.VMEM(exp_gate.shape[1:], bf16),
            pltpu.VMEM(exp_up.shape[1:], bf16),
            pltpu.VMEM(exp_down.shape[1:], bf16),
            pltpu.VMEM(sh_gate.shape, bf16),
            pltpu.VMEM(sh_up.shape, bf16),
            pltpu.VMEM(sh_down.shape, bf16),
            pltpu.VMEM((halo_rows, channels), bf16),
            pltpu.VMEM((halo_rows, channels), bf16),
            pltpu.VMEM((halo_rows + tok_rows, channels), f32),
            pltpu.VMEM((tok_rows, channels), f32),
            pltpu.VMEM((2, tok_rows), f32),
            pltpu.VMEM((3, 2, tok_rows), f32),
            pltpu.VMEM((tok_rows, channels), bf16),
            pltpu.VMEM((tok_rows, channels), bf16),
            pltpu.VMEM((channels, half_width), bf16),
            pltpu.VMEM((tok_rows, half_width), f32),
            pltpu.VMEM((tok_rows, half_width), bf16),
            pltpu.VMEM((tok_rows, half_width), bf16),
            pltpu.VMEM((2, count, tok_rows, half_width), bf16),
            pltpu.VMEM((tok_rows, model_width), bf16),
            pltpu.VMEM((4, count, tok_rows, part_hidden), bf16),
            pltpu.VMEM((4, tok_rows, shared_width), bf16),
            pltpu.VMEM((count, tok_rows, col_width), bf16),
            pltpu.VMEM((count, tok_rows, col_width), bf16),
            pltpu.VMEM((tok_rows, col_width), f32),
            dma((17,)),
            dma((2,)),
            dma((3,)),
            dma((3,)),
            dma((4,)),
            dma((ROW_CUTS,)),
            dma((ROW_CUTS,)),
            dma((levels * ROW_CUTS,)),
            dma((levels * ROW_CUTS,)),
            dma((levels * ROW_CUTS,)),
            dma((pieces,)),
            dma((pieces,)),
            dma((pieces,)),
            dma((pieces,)),
            dma((pieces,)),
            dma((pieces,)),
            dma((pieces,)),
            dma((pieces,)),
            dma((pieces,)),
            dma((3,)),
            dma((3,)),
            dma((pieces,)),
            dma((pieces,)),
        ],
        compiler_params=pltpu.CompilerParams(
            collective_id=0, has_side_effects=True, vmem_limit_bytes=56 * 1024 * 1024
        ),
    )(*operands)


def body(*args):
    tok_rows = args[0].shape[0]
    top_count = args[9].shape[1]
    local_experts = args[11].shape[0]
    experts_all = local_experts * lax.axis_size("sp")
    capacity = 2 * tok_rows * top_count // experts_all
    if (
        local_experts == 1
        and lax.axis_size("tp") == 4
        and lax.axis_size("sp") == 8
        and capacity >= tok_rows
    ):
        return body_dense(*args)
    return body_slots(*args)


def solution(mesh):
    in_specs = (
        P("sp", None),
        P("sp", "tp"),
        P("sp", "tp"),
        P(None, "tp"),
        P("tp"),
        P("tp"),
        P("tp"),
        P("tp", None),
        P(),
        P("sp", None),
        P("sp", None),
        P("sp", None, "tp"),
        P("sp", None, "tp"),
        P("sp", None, "tp"),
        P(None, "tp"),
        P(None, "tp"),
        P(None, "tp"),
    )
    out_specs = P("sp", "tp")
    return jax.shard_map(body, mesh=mesh, in_specs=in_specs, out_specs=out_specs, check_vma=False)
```

```python
import functools

import jax
import jax.numpy as jnp
from jax import lax
from jax.experimental import pallas as pl
from jax.experimental.pallas import tpu as pltpu
from jax.sharding import PartitionSpec as P

LN_EPS = 1e-05
RMS_EPS = 1e-06


def shifted(value, axis, by):
    size = lax.axis_size(axis)
    pairs = [(i, i + by) for i in range(size) if 0 <= i + by < size]
    return lax.ppermute(value, axis, pairs)


def body_slots(
    resid,
    a_val,
    a_gate,
    conv_kernel,
    conv_bias,
    ln_gain,
    ln_bias,
    w_out,
    ffn_gain,
    routes,
    route_weights,
    exp_gate,
    exp_up,
    exp_down,
    sh_gate,
    sh_up,
    sh_down,
):
    tp_count = lax.axis_size("tp")
    tp_place = lax.axis_index("tp")
    sp_count = lax.axis_size("sp")
    tok_rows = resid.shape[0]
    model_width = resid.shape[1]
    col_width = model_width // tp_count
    col_start = tp_place * col_width
    conv_span = conv_kernel.shape[0]
    channels_all = a_val.shape[1] * tp_count
    gated_in = (a_val.astype(jnp.float32) * jax.nn.sigmoid(a_gate.astype(jnp.float32))).astype(
        jnp.bfloat16
    )
    before = shifted(gated_in[tok_rows - (conv_span - 1) :], "sp", 1)
    padded = jnp.concatenate([before, gated_in], axis=0).astype(jnp.float32)
    kernel = conv_kernel.astype(jnp.float32)

    def add_tap(offset, running):
        window_rows = lax.dynamic_slice_in_dim(padded, offset, tok_rows, 0)
        return running + lax.dynamic_slice_in_dim(kernel, offset, 1, 0) * window_rows

    start_sum = jnp.broadcast_to(conv_bias[None, :], gated_in.shape)
    conv_out = lax.fori_loop(0, conv_span, add_tap, start_sum)
    row_sums = lax.psum((jnp.sum(conv_out, axis=1), jnp.sum(conv_out * conv_out, axis=1)), "tp")
    channel_mean = row_sums[0] / channels_all
    channel_var = row_sums[1] / channels_all - channel_mean * channel_mean
    scaled = (conv_out - channel_mean[:, None]) * lax.rsqrt(
        channel_var[:, None] + LN_EPS
    ) * ln_gain[None, :] + ln_bias[None, :]
    mixed_out = jax.nn.silu(scaled).astype(jnp.bfloat16)
    partial_proj = jnp.dot(mixed_out, w_out, preferred_element_type=jnp.float32)
    projected = lax.psum(partial_proj, "tp")
    middle = (resid.astype(jnp.float32) + projected).astype(jnp.bfloat16)
    middle_f = middle.astype(jnp.float32)
    inverse = lax.rsqrt(jnp.mean(middle_f * middle_f, axis=1, keepdims=True) + RMS_EPS)
    normed = (middle_f * inverse * ffn_gain[None, :]).astype(jnp.bfloat16)
    middle_cols = lax.dynamic_slice_in_dim(middle, col_start, col_width, 1)
    shared_gate = jnp.dot(normed, sh_gate, preferred_element_type=jnp.float32)
    shared_up = jnp.dot(normed, sh_up, preferred_element_type=jnp.float32)
    shared_hidden = (jax.nn.silu(shared_gate) * shared_up).astype(jnp.bfloat16)
    weight_rows = sh_down
    shared = jnp.dot(
        lax.all_gather(shared_hidden, "tp", axis=1, tiled=True),
        weight_rows,
        preferred_element_type=jnp.float32,
    )
    top_count = routes.shape[1]
    local_experts = exp_gate.shape[0]
    experts_all = local_experts * sp_count
    capacity = max(2 * tok_rows * top_count // experts_all, tp_count)
    pair_count = tok_rows * top_count
    chosen = routes.reshape(pair_count)
    one_hot = (chosen[:, None] == jnp.arange(experts_all, dtype=jnp.int32)[None, :]).astype(
        jnp.int32
    )
    earlier = jnp.cumsum(one_hot, axis=0) - one_hot
    place_in = jnp.sum(earlier * one_hot, axis=1)
    slot_of = chosen * capacity + place_in
    owner_ids = (
        jnp.zeros((experts_all * capacity,), jnp.int32)
        .at[slot_of]
        .set(jnp.arange(pair_count, dtype=jnp.int32) + 1)
    )
    owner_grid = owner_ids.reshape(sp_count, local_experts, capacity)
    part_slots = capacity // tp_count
    own_owners = lax.dynamic_slice_in_dim(owner_grid, tp_place * part_slots, part_slots, 2)
    source_row = jnp.maximum(own_owners - 1, 0) // top_count
    taken = normed[source_row.reshape(-1)].reshape(own_owners.shape + (model_width,))
    landed = lax.all_to_all(
        jnp.where((own_owners > 0)[..., None], taken, jnp.zeros((), jnp.bfloat16)),
        "sp",
        split_axis=0,
        concat_axis=0,
        tiled=True,
    )
    arrived = lax.all_gather(landed, "tp", axis=2, tiled=True)
    gate_part = jnp.einsum("sxcd,xdf->sxcf", arrived, exp_gate, preferred_element_type=jnp.float32)
    up_part = jnp.einsum("sxcd,xdf->sxcf", arrived, exp_up, preferred_element_type=jnp.float32)
    expert_hidden = (jax.nn.silu(gate_part) * up_part).astype(jnp.bfloat16)
    weight_rows = exp_down
    expert_sum = jnp.einsum(
        "sxcf,xfd->sxcd",
        lax.all_gather(expert_hidden, "tp", axis=3, tiled=True),
        weight_rows,
        preferred_element_type=jnp.float32,
    )
    expert_out = expert_sum.astype(jnp.bfloat16)
    returned = lax.all_to_all(expert_out, "sp", split_axis=0, concat_axis=0, tiled=True)
    flat_out = returned.reshape(experts_all * capacity, col_width)
    picked = flat_out[slot_of].astype(jnp.float32).reshape(tok_rows, top_count, col_width)
    routed = jnp.sum(picked * route_weights[:, :, None], axis=1)
    return (middle_cols.astype(jnp.float32) + shared + routed).astype(jnp.bfloat16)


ROW_CUTS = 4


def silu(value):
    return value / (1.0 + jnp.exp(-value))


def layer_kernel(
    levels,
    resid_hbm,
    a_val_hbm,
    a_gate_hbm,
    taps_hbm,
    conv_bias_hbm,
    ln_gain_hbm,
    ln_bias_hbm,
    w_out_hbm,
    ffn_gain_hbm,
    routes_hbm,
    route_weights_hbm,
    exp_gate_hbm,
    exp_up_hbm,
    exp_down_hbm,
    sh_gate_hbm,
    sh_up_hbm,
    sh_down_hbm,
    out_ref,
    resid_ref,
    a_val_ref,
    a_gate_ref,
    taps_ref,
    conv_bias_ref,
    ln_gain_ref,
    ln_bias_ref,
    w_out_ref,
    ffn_gain_ref,
    routes_ref,
    route_weights_ref,
    gate_ref,
    up_ref,
    down_ref,
    sh_gate_ref,
    sh_up_ref,
    sh_down_ref,
    halo_out,
    halo_in,
    padded_ref,
    conv_ref,
    stat_out,
    stat_in,
    mix_out,
    mix_in,
    w_in,
    keep_ref,
    chip_out,
    chip_in,
    rows_ref,
    normed_ref,
    hidden_ref,
    shared_ref,
    part_ref,
    back_ref,
    sum_ref,
    load_sem,
    halo_sem,
    stat_send,
    stat_recv,
    mix_sem,
    chip_send,
    chip_recv,
    up_sem,
    low_sem,
    side_sem,
    core_sem,
    main_recv,
    core_recv,
    far_send,
    far_recv,
    near_send,
    near_recv,
    relay_send,
    relay_recv,
    shared_send,
    shared_recv,
    back_send,
    back_recv,
):
    count = 2 * levels
    me = lax.axis_index("sp")
    tp_place = lax.axis_index("tp")
    level, side = me // 2, me % 2
    row, core = tp_place // 2, tp_place % 2
    core_place = row * 2 + (1 - core)
    row_place = (1 - row) * 2 + core
    core_peer = {"tp": core_place}
    row_peer = {"tp": row_place}
    far_peer = {"tp": (1 - row) * 2 + (1 - core)}
    side_peer = {"sp": level * 2 + (1 - side)}
    mesh_ids = pl.DeviceIdType.MESH
    f32, bf16 = jnp.float32, jnp.bfloat16
    tok_rows, half_width = resid_ref.shape
    model_width = 2 * half_width
    col_width = out_ref.shape[1]
    span = taps_ref.shape[0]
    halo_rows = halo_in.shape[0]
    channels_all = 4 * a_val_ref.shape[1]
    part_hidden = gate_ref.shape[1]
    cut_rows = tok_rows // ROW_CUTS

    half_at = pl.ds(pl.multiple_of(core * half_width, half_width), half_width)
    pairs = [
        (a_val_hbm, a_val_ref),
        (a_gate_hbm, a_gate_ref),
        (taps_hbm, taps_ref),
        (conv_bias_hbm, conv_bias_ref),
        (ln_gain_hbm, ln_gain_ref),
        (ln_bias_hbm, ln_bias_ref),
        (w_out_hbm.at[:, half_at], w_out_ref),
        (resid_hbm.at[:, half_at], resid_ref),
        (ffn_gain_hbm, ffn_gain_ref),
        (exp_gate_hbm, gate_ref),
        (exp_up_hbm, up_ref),
        (sh_gate_hbm, sh_gate_ref),
        (sh_up_hbm, sh_up_ref),
        (exp_down_hbm, down_ref),
        (sh_down_hbm, sh_down_ref),
        (routes_hbm, routes_ref),
        (route_weights_hbm, route_weights_ref),
    ]
    loads = [
        pltpu.make_async_copy(src, dst, load_sem.at[at]) for at, (src, dst) in enumerate(pairs)
    ]
    for load in loads:
        load.start()

    barrier = pltpu.get_barrier_semaphore()

    def greet(peer):
        pl.semaphore_signal(barrier, inc=1, device_id=peer, device_id_type=mesh_ids)

    across = ((side == 0) & (level > 0)) | ((side == 1) & (level < levels - 1))
    for peer in (core_peer, row_peer, far_peer, side_peer):
        greet(peer)

    @pl.when(level > 0)
    def _():
        greet({"sp": me - 2})

    @pl.when(level < levels - 1)
    def _():
        greet({"sp": me + 2})

    @pl.when(across)
    def _():
        greet({"sp": me + 2 * side - 1})

    def remote(src, dst, send, recv, where):
        return pltpu.make_async_remote_copy(
            src_ref=src, dst_ref=dst, send_sem=send, recv_sem=recv, device_id=where, device_id_type=mesh_ids
        )

    for load in loads[:4]:
        load.wait()
    gated = (a_val_ref[...].astype(f32) / (1.0 + jnp.exp(-a_gate_ref[...].astype(f32)))).astype(bf16)
    halo_out[...] = gated[tok_rows - halo_rows :]
    padded_ref[halo_rows:, :] = gated.astype(f32)
    taps = taps_ref[...].astype(f32)

    def convolve(first, size):
        total = jnp.broadcast_to(conv_bias_ref[...], (size, gated.shape[1]))
        for tap in range(span):
            at = first + tap + halo_rows - (span - 1)
            total = total + taps[tap : tap + 1] * padded_ref[at : at + size, :]
        conv_ref[first : first + size, :] = total

    diagonal = lax.broadcasted_iota(jnp.int32, (tok_rows, tok_rows), 0) == lax.broadcasted_iota(
        jnp.int32, (tok_rows, tok_rows), 1
    )

    def lying(column, first):
        mask = diagonal[first : first + column.shape[0]]
        return jnp.sum(jnp.where(mask, column, 0.0), axis=0, keepdims=True)

    def standing(line, first, size):
        mask = diagonal[first : first + size]
        return jnp.sum(jnp.where(mask, line, 0.0), axis=1, keepdims=True)

    def measure(first, size, part):
        rows = conv_ref[first : first + size, :]
        stat_out[part, 0:1, :] = lying(jnp.sum(rows, axis=1, keepdims=True), first)
        stat_out[part, 1:2, :] = lying(jnp.sum(rows * rows, axis=1, keepdims=True), first)

    stats = [
        [
            remote(
                stat_out.at[part],
                stat_in.at[part, at],
                stat_send.at[part * 3 + at],
                stat_recv.at[part * 3 + at],
                peer,
            )
            for at, peer in enumerate((core_peer, row_peer, far_peer))
        ]
        for part in range(2)
    ]
    rest = tok_rows - halo_rows
    convolve(halo_rows, rest)
    measure(halo_rows, rest, 0)

    has_below = (level + levels - 2) // (levels - 1)
    has_above = (2 * levels - 3 - level) // (levels - 1)
    has_across = has_below + side * (has_above - has_below)
    pl.semaphore_wait(barrier, 4 + has_below + has_above + has_across)
    give_at = pl.ds(pl.multiple_of((1 - core) * half_width, half_width), half_width)
    w_swap = remote(w_out_hbm.at[:, give_at], w_in, mix_sem.at[0], mix_sem.at[1], core_peer)
    halo = lambda where: remote(halo_out, halo_in, halo_sem.at[0], halo_sem.at[1], {"sp": where})

    @pl.when(me < count - 1)
    def _():
        halo(me + 1).start()

    for copy in stats[0]:
        copy.start()
    w_swap.start()

    @pl.when(me == 0)
    def _():
        padded_ref[:halo_rows, :] = jnp.zeros((halo_rows, gated.shape[1]), f32)

    @pl.when(me > 0)
    def _():
        halo(me).wait_recv()
        padded_ref[:halo_rows, :] = halo_in[...].astype(f32)

    convolve(0, halo_rows)
    measure(0, halo_rows, 1)
    for copy in stats[1]:
        copy.start()
    for load in loads[4:9]:
        load.wait()

    def cut(at):
        return pl.ds(at * cut_rows, cut_rows)

    mixes = [
        remote(
            mix_out.at[some], mix_in.at[some], mix_sem.at[2 + part], mix_sem.at[4 + part], core_peer
        )
        for part, some in enumerate((pl.ds(halo_rows, rest), pl.ds(0, halo_rows)))
    ]
    chips = [
        remote(
            chip_out.at[cut(at)], chip_in.at[cut(at)], chip_send.at[at], chip_recv.at[at], row_peer
        )
        for at in range(ROW_CUTS)
    ]

    def project(first, size, part):
        some = slice(first, first + size)
        for copy in stats[part]:
            copy.wait_recv()
        sums = (stat_out[part] + stat_in[part, 0]) + (stat_in[part, 1] + stat_in[part, 2])
        channel_mean = standing(sums[0:1], first, size) / channels_all
        channel_var = standing(sums[1:2], first, size) / channels_all - channel_mean * channel_mean
        scaled = (conv_ref[some, :] - channel_mean) * lax.rsqrt(channel_var + LN_EPS) * ln_gain_ref[
            ...
        ] + ln_bias_ref[...]
        mix_out[some, :] = silu(scaled).astype(bf16)
        mixes[part].start()
        keep_ref[some, :] = jnp.dot(mix_out[some, :], w_out_ref[...], preferred_element_type=f32)
        if part == 0:
            w_swap.wait_recv()
        mixes[part].wait_recv()
        for at in range((first + size) // cut_rows - 1, first // cut_rows - 1, -1):
            chip_sum = keep_ref[cut(at), :] + jnp.dot(
                mix_in[cut(at), :], w_in[...], preferred_element_type=f32
            )
            keep_ref[cut(at), :] = chip_sum
            chip_out[cut(at), :] = chip_sum.astype(bf16)
            chips[at].start()

    project(halo_rows, rest, 0)
    project(0, halo_rows, 1)

    def block(half, at, piece):
        return rows_ref.at[half, at, cut(piece)]

    def up_copy(origin, piece):
        at = origin * 2 + side
        sem = origin * ROW_CUTS + piece
        spot = block(core, at, piece)
        return remote(spot, spot, up_sem.at[sem], main_recv.at[at * ROW_CUTS + piece], {"sp": me + 2})

    def low_copy(origin, piece):
        at = origin * 2 + side
        sem = origin * ROW_CUTS + piece
        spot = block(core, at, piece)
        return remote(spot, spot, low_sem.at[sem], main_recv.at[at * ROW_CUTS + piece], {"sp": me - 2})

    def side_copy(origin, piece):
        at = origin * 2 + side
        sem = origin * ROW_CUTS + piece
        spot = block(core, at, piece)
        return remote(spot, spot, side_sem.at[sem], main_recv.at[at * ROW_CUTS + piece], side_peer)

    def core_copy(at, piece):
        sem = at * ROW_CUTS + piece
        spot = block(core, at, piece)
        return remote(spot, spot, core_sem.at[sem], core_recv.at[sem], core_peer)

    def landed(at, piece):
        spot = block(core, at, piece)
        sem = at * ROW_CUTS + piece
        remote(spot, spot, core_sem.at[sem], main_recv.at[sem], core_peer).wait_recv()

    def crossed(at, piece):
        spot = block(1 - core, at, piece)
        sem = at * ROW_CUTS + piece
        remote(spot, spot, core_sem.at[sem], core_recv.at[sem], core_peer).wait_recv()

    def settle(piece):
        chips[piece].wait_recv()
        total = keep_ref[cut(piece), :] + chip_in[cut(piece), :].astype(f32)
        rows_ref[core, me, cut(piece), :] = (resid_ref[cut(piece), :].astype(f32) + total).astype(bf16)
        core_copy(me, piece).start()
        side_copy(level, piece).start()

        @pl.when(level < levels - 1)
        def _():
            up_copy(level, piece).start()

        @pl.when(level > 0)
        def _():
            low_copy(level, piece).start()

    def normalise(at, some):
        low = rows_ref[0, at, some, :].astype(f32)
        high = rows_ref[1, at, some, :].astype(f32)
        power = jnp.sum(low * low, axis=1, keepdims=True) + jnp.sum(high * high, axis=1, keepdims=True)
        inverse = lax.rsqrt(power / model_width + RMS_EPS)
        normed_ref[some, :half_width] = (low * inverse * ffn_gain_ref[:, :half_width]).astype(bf16)
        normed_ref[some, half_width:] = (high * inverse * ffn_gain_ref[:, half_width:]).astype(bf16)

    def hidden_copy(place, at, run, send, recv, peer):
        spot = hidden_ref.at[place, at, pl.ds(*run)]
        sem = at * ROW_CUTS + run[0] // cut_rows
        return remote(spot, spot, send.at[sem], recv.at[sem], peer)

    def far_copy(at, run):
        return hidden_copy(tp_place, at, run, far_send, far_recv, row_peer)

    def near_copy(at, run):
        return hidden_copy(tp_place, at, run, near_send, near_recv, core_peer)

    def relay_copy(at, run):
        return hidden_copy(row_place, at, run, relay_send, relay_recv, core_peer)

    shared_far = remote(
        shared_ref.at[tp_place], shared_ref.at[tp_place], shared_send.at[0], shared_recv.at[0], row_peer
    )
    shared_near = remote(
        shared_ref.at[tp_place], shared_ref.at[tp_place], shared_send.at[1], shared_recv.at[1], core_peer
    )
    shared_relay = remote(
        shared_ref.at[row_place], shared_ref.at[row_place], shared_send.at[2], shared_recv.at[2], core_peer
    )

    half_rows = tok_rows // 2
    falling = range(ROW_CUTS - 1, -1, -1)
    opening = (half_rows, half_rows)
    closing = (0, half_rows)
    halves = (opening, closing)
    singles = tuple((piece * cut_rows, cut_rows) for piece in falling[: ROW_CUTS // 2])

    def hide(at, first, size, runs):
        some = pl.ds(first, size)
        normalise(at, some)
        step = 256
        for left in range(0, part_hidden, step):
            wide = slice(left, left + step)
            gate_part = jnp.dot(normed_ref[some, :], gate_ref[:, wide], preferred_element_type=f32)
            up_part = jnp.dot(normed_ref[some, :], up_ref[:, wide], preferred_element_type=f32)
            hidden_ref[tp_place, at, some, wide] = (silu(gate_part) * up_part).astype(bf16)
        for run in runs:
            far_copy(at, run).start()
        for run in runs:
            near_copy(at, run).start()

    def gather_hide(at, first, size, runs):
        for piece in range((first + size) // cut_rows - 1, first // cut_rows - 1, -1):
            crossed(at, piece)
        hide(at, first, size, runs)

    def down_part(at, some, place):
        return jnp.dot(
            hidden_ref[place, at, some, :],
            down_ref[pl.ds(pl.multiple_of(place * part_hidden, part_hidden), part_hidden), :],
            preferred_element_type=f32,
        )

    def back_copy(at, half):
        some = pl.ds(half * half_rows, half_rows)
        return remote(
            part_ref.at[at, some],
            back_ref.at[me, some],
            back_send.at[at * 2 + half],
            back_recv.at[me * 2 + half],
            {"sp": at},
        )

    def relay(at, run):
        far_copy(at, run).wait_recv()
        relay_copy(at, run).start()

    def finish(at, first, size, runs):
        for run in runs:
            relay(at, run)
        for run in runs:
            near_copy(at, run).wait_recv()
        for run in runs:
            relay_copy(at, run).wait_recv()
        some = pl.ds(first, size)
        total = (down_part(at, some, 0) + down_part(at, some, 1)) + (
            down_part(at, some, 2) + down_part(at, some, 3)
        )
        part_ref[at, some, :] = total.astype(bf16)
        for half in range((first + size) // half_rows - 1, first // half_rows - 1, -1):
            back_copy(at, half).start()

    def pass_on(step, piece):
        below = level - step
        above = level + step

        @pl.when(below >= 0)
        def _():
            landed(below * 2 + side, piece)

            @pl.when(level < levels - 1)
            def _():
                up_copy(below, piece).start()

            side_copy(below, piece).start()
            core_copy(below * 2 + side, piece).start()

        @pl.when(above < levels)
        def _():
            landed(above * 2 + side, piece)

            @pl.when(level > 0)
            def _():
                low_copy(above, piece).start()

            side_copy(above, piece).start()
            core_copy(above * 2 + side, piece).start()

    def from_side(at):
        for piece in falling:
            landed(at, piece)
            core_copy(at, piece).start()

    upper = (2 * level) // levels
    inner = level + upper * (levels - 1 - 2 * level)

    def visited(outer_way, inner_way):
        mirrored = outer_way[0] + inner * (inner_way[0] - outer_way[0])
        at_level = mirrored + upper * (levels - 1 - 2 * mirrored)
        return at_level * 2 + lax.rem(side + outer_way[1], 2)

    outer_order = ((1, 0), (2, 0), (3, 0), (2, 1), (3, 1), (1, 1))
    inner_order = ((0, 0), (2, 0), (3, 0), (2, 1), (0, 1), (3, 1))
    next_door, *visits = [visited(*ways) for ways in zip(outer_order, inner_order)]
    beside = level * 2 + (1 - side)

    def forward(piece):
        landed(beside, piece)
        core_copy(beside, piece).start()
        pass_on(1, piece)

    settle(falling[0])
    settle(falling[1])
    for load in loads[9:11]:
        load.wait()
    gather_hide(me, *singles[0], singles[:1])
    settle(falling[2])
    forward(falling[0])
    gather_hide(me, *singles[1], singles[1:])
    settle(falling[3])
    forward(falling[1])
    gather_hide(next_door, *singles[0], singles[:1])
    gather_hide(next_door, *singles[1], singles[1:])
    forward(falling[2])
    gather_hide(beside, *opening, (opening,))
    forward(falling[3])
    gather_hide(next_door, *closing, (closing,))
    for load in loads[11:]:
        load.wait()
    for piece in falling:
        pass_on(2, piece)
    gather_hide(visits[0], 0, tok_rows, halves)
    for piece in falling:
        pass_on(3, piece)
    gather_hide(visits[1], 0, tok_rows, halves)
    from_side(visits[2])
    for run in singles:
        relay(me, run)
    finish(next_door, 0, tok_rows, singles + (closing,))
    gather_hide(visits[2], 0, tok_rows, halves)
    from_side(visits[3])
    finish(beside, *opening, (opening,))
    finish(visits[0], 0, tok_rows, halves)
    gather_hide(visits[3], 0, tok_rows, halves)
    from_side(visits[4])
    finish(visits[1], 0, tok_rows, halves)

    for piece in falling[2:]:
        crossed(me, piece)
    whole = pl.ds(0, tok_rows)
    normalise(me, whole)
    shared_gate = jnp.dot(normed_ref[...], sh_gate_ref[...], preferred_element_type=f32)
    shared_up = jnp.dot(normed_ref[...], sh_up_ref[...], preferred_element_type=f32)
    shared_ref[tp_place] = (silu(shared_gate) * shared_up).astype(bf16)
    shared_far.start()
    shared_near.start()

    gather_hide(visits[4], 0, tok_rows, halves)
    finish(visits[2], 0, tok_rows, halves)
    gather_hide(beside, *closing, (closing,))
    hide(me, *closing, (closing,))

    middle_cols = rows_ref[row, me, :, pl.ds(pl.multiple_of(core * col_width, col_width), col_width)]
    shared_far.wait_recv()
    shared_relay.start()
    shared_near.wait_recv()
    shared_relay.wait_recv()
    total = middle_cols.astype(f32)
    shared_width = shared_ref.shape[2]
    for place in range(4):
        total = total + jnp.dot(
            shared_ref[place],
            sh_down_ref[place * shared_width : (place + 1) * shared_width, :],
            preferred_element_type=f32,
        )
    sum_ref[...] = total
    finish(visits[3], 0, tok_rows, halves)
    finish(visits[4], 0, tok_rows, halves)
    finish(beside, *closing, (closing,))

    for run in singles + (closing,):
        near_copy(me, run).wait_recv()
    for run in singles:
        relay_copy(me, run).wait_recv()
    own_part = down_part(me, whole, tp_place) + down_part(me, whole, core_place)
    relay(me, closing)
    own_part = own_part + down_part(me, whole, row_place)
    relay_copy(me, closing).wait_recv()
    own_part = own_part + down_part(me, whole, (1 - row) * 2 + (1 - core))
    part_ref[me] = own_part.astype(bf16)
    total = sum_ref[...]
    routes = routes_ref[...]
    route_weights = route_weights_ref[...]
    def weight_of(at):
        line = jnp.sum(jnp.where(routes == at, route_weights, 0.0), axis=0, keepdims=True)
        return standing(line, 0, tok_rows)

    total = total + weight_of(me) * part_ref[me].astype(f32)
    for step in range(1, count):
        at = lax.rem(me + step, count)
        for half in range(2):
            some = pl.ds(half * half_rows, half_rows)
            sem = at * 2 + half
            remote(
                part_ref.at[at, some], back_ref.at[at, some], back_send.at[sem], back_recv.at[sem], core_peer
            ).wait_recv()
        total = total + weight_of(at) * back_ref[at].astype(f32)
    out_ref[...] = total.astype(bf16)

    @pl.when(me < count - 1)
    def _():
        halo(me + 1).wait_send()

    for copy in stats[0] + stats[1] + mixes + chips + [w_swap, shared_far, shared_near, shared_relay]:
        copy.wait_send()

    @pl.loop(0, levels)
    def _(origin):
        for piece in range(ROW_CUTS):
            side_copy(origin, piece).wait_send()

            @pl.when((level < levels - 1) & (origin <= level))
            def _():
                up_copy(origin, piece).wait_send()

            @pl.when((level > 0) & (origin >= level))
            def _():
                low_copy(origin, piece).wait_send()

    split = singles + (closing,)
    trips = [(me, split), (next_door, split), (beside, halves)] + [(at, halves) for at in visits]
    for at, runs in trips:
        for run in runs:
            far_copy(at, run).wait_send()
            near_copy(at, run).wait_send()
            relay_copy(at, run).wait_send()

    @pl.loop(0, count)
    def _(at):
        for piece in range(ROW_CUTS):
            core_copy(at, piece).wait_send()

        @pl.when(at != me)
        def _():
            for half in range(2):
                back_copy(at, half).wait_send()


def body_dense(
    resid,
    a_val,
    a_gate,
    conv_kernel,
    conv_bias,
    ln_gain,
    ln_bias,
    w_out,
    ffn_gain,
    routes,
    route_weights,
    exp_gate,
    exp_up,
    exp_down,
    sh_gate,
    sh_up,
    sh_down,
):
    count = lax.axis_size("sp")
    levels = count // 2
    tok_rows, model_width = resid.shape
    half_width = model_width // 2
    channels = a_val.shape[1]
    part_hidden = exp_gate.shape[2]
    col_width = exp_down.shape[2]
    shared_width = sh_gate.shape[1]
    top_count = routes.shape[1]
    halo_rows = tok_rows // ROW_CUTS
    vmem = pl.BlockSpec(memory_space=pltpu.VMEM)
    hbm = pl.BlockSpec(memory_space=pltpu.HBM)
    f32, bf16 = jnp.float32, jnp.bfloat16
    dma = pltpu.SemaphoreType.DMA
    operands = (
        resid,
        a_val,
        a_gate,
        conv_kernel,
        conv_bias.reshape(1, -1),
        ln_gain.reshape(1, -1),
        ln_bias.reshape(1, -1),
        w_out,
        ffn_gain.reshape(1, -1),
        routes.T,
        route_weights.T,
        exp_gate[0],
        exp_up[0],
        exp_down[0],
        sh_gate,
        sh_up,
        sh_down,
    )
    pieces = count * ROW_CUTS
    return pl.pallas_call(
        functools.partial(layer_kernel, levels),
        out_shape=jax.ShapeDtypeStruct((tok_rows, col_width), bf16),
        in_specs=[hbm] * len(operands),
        out_specs=vmem,
        scratch_shapes=[
            pltpu.VMEM((tok_rows, half_width), bf16),
            pltpu.VMEM(a_val.shape, bf16),
            pltpu.VMEM(a_gate.shape, bf16),
            pltpu.VMEM(conv_kernel.shape, bf16),
            pltpu.VMEM((1, channels), f32),
            pltpu.VMEM((1, channels), f32),
            pltpu.VMEM((1, channels), f32),
            pltpu.VMEM((channels, half_width), bf16),
            pltpu.VMEM((1, model_width), f32),
            pltpu.VMEM((top_count, tok_rows), jnp.int32),
            pltpu.VMEM((top_count, tok_rows), f32),
            pltpu.VMEM(exp_gate.shape[1:], bf16),
            pltpu.VMEM(exp_up.shape[1:], bf16),
            pltpu.VMEM(exp_down.shape[1:], bf16),
            pltpu.VMEM(sh_gate.shape, bf16),
            pltpu.VMEM(sh_up.shape, bf16),
            pltpu.VMEM(sh_down.shape, bf16),
            pltpu.VMEM((halo_rows, channels), bf16),
            pltpu.VMEM((halo_rows, channels), bf16),
            pltpu.VMEM((halo_rows + tok_rows, channels), f32),
            pltpu.VMEM((tok_rows, channels), f32),
            pltpu.VMEM((2, 2, tok_rows), f32),
            pltpu.VMEM((2, 3, 2, tok_rows), f32),
            pltpu.VMEM((tok_rows, channels), bf16),
            pltpu.VMEM((tok_rows, channels), bf16),
            pltpu.VMEM((channels, half_width), bf16),
            pltpu.VMEM((tok_rows, half_width), f32),
            pltpu.VMEM((tok_rows, half_width), bf16),
            pltpu.VMEM((tok_rows, half_width), bf16),
            pltpu.VMEM((2, count, tok_rows, half_width), bf16),
            pltpu.VMEM((tok_rows, model_width), bf16),
            pltpu.VMEM((4, count, tok_rows, part_hidden), bf16),
            pltpu.VMEM((4, tok_rows, shared_width), bf16),
            pltpu.VMEM((count, tok_rows, col_width), bf16),
            pltpu.VMEM((count, tok_rows, col_width), bf16),
            pltpu.VMEM((tok_rows, col_width), f32),
            dma((17,)),
            dma((2,)),
            dma((6,)),
            dma((6,)),
            dma((6,)),
            dma((ROW_CUTS,)),
            dma((ROW_CUTS,)),
            dma((levels * ROW_CUTS,)),
            dma((levels * ROW_CUTS,)),
            dma((levels * ROW_CUTS,)),
            dma((pieces,)),
            dma((pieces,)),
            dma((pieces,)),
            dma((pieces,)),
            dma((pieces,)),
            dma((pieces,)),
            dma((pieces,)),
            dma((pieces,)),
            dma((pieces,)),
            dma((3,)),
            dma((3,)),
            dma((2 * count,)),
            dma((2 * count,)),
        ],
        compiler_params=pltpu.CompilerParams(
            collective_id=0, has_side_effects=True, vmem_limit_bytes=56 * 1024 * 1024
        ),
    )(*operands)


def body(*args):
    tok_rows = args[0].shape[0]
    top_count = args[9].shape[1]
    local_experts = args[11].shape[0]
    experts_all = local_experts * lax.axis_size("sp")
    capacity = 2 * tok_rows * top_count // experts_all
    if (
        local_experts == 1
        and lax.axis_size("tp") == 4
        and lax.axis_size("sp") == 8
        and ROW_CUTS * (args[3].shape[0] - 1) <= tok_rows
        and capacity >= tok_rows
    ):
        return body_dense(*args)
    return body_slots(*args)


def solution(mesh):
    in_specs = (
        P("sp", None),
        P("sp", "tp"),
        P("sp", "tp"),
        P(None, "tp"),
        P("tp"),
        P("tp"),
        P("tp"),
        P("tp", None),
        P(),
        P("sp", None),
        P("sp", None),
        P("sp", None, "tp"),
        P("sp", None, "tp"),
        P("sp", None, "tp"),
        P(None, "tp"),
        P(None, "tp"),
        P(None, "tp"),
    )
    out_specs = P("sp", "tp")
    return jax.shard_map(body, mesh=mesh, in_specs=in_specs, out_specs=out_specs, check_vma=False)
```

```python
import functools

import jax
import jax.numpy as jnp
from jax import lax
from jax.experimental import pallas as pl
from jax.experimental.pallas import tpu as pltpu
from jax.sharding import PartitionSpec as P

LN_EPS = 1e-05
RMS_EPS = 1e-06


def shifted(value, axis, by):
    size = lax.axis_size(axis)
    pairs = [(i, i + by) for i in range(size) if 0 <= i + by < size]
    return lax.ppermute(value, axis, pairs)


def body_slots(
    resid,
    a_val,
    a_gate,
    conv_kernel,
    conv_bias,
    ln_gain,
    ln_bias,
    w_out,
    ffn_gain,
    routes,
    route_weights,
    exp_gate,
    exp_up,
    exp_down,
    sh_gate,
    sh_up,
    sh_down,
):
    tp_count = lax.axis_size("tp")
    tp_place = lax.axis_index("tp")
    sp_count = lax.axis_size("sp")
    tok_rows = resid.shape[0]
    model_width = resid.shape[1]
    col_width = model_width // tp_count
    col_start = tp_place * col_width
    conv_span = conv_kernel.shape[0]
    channels_all = a_val.shape[1] * tp_count
    gated_in = (a_val.astype(jnp.float32) * jax.nn.sigmoid(a_gate.astype(jnp.float32))).astype(
        jnp.bfloat16
    )
    before = shifted(gated_in[tok_rows - (conv_span - 1) :], "sp", 1)
    padded = jnp.concatenate([before, gated_in], axis=0).astype(jnp.float32)
    kernel = conv_kernel.astype(jnp.float32)

    def add_tap(offset, running):
        window_rows = lax.dynamic_slice_in_dim(padded, offset, tok_rows, 0)
        return running + lax.dynamic_slice_in_dim(kernel, offset, 1, 0) * window_rows

    start_sum = jnp.broadcast_to(conv_bias[None, :], gated_in.shape)
    conv_out = lax.fori_loop(0, conv_span, add_tap, start_sum)
    row_sums = lax.psum((jnp.sum(conv_out, axis=1), jnp.sum(conv_out * conv_out, axis=1)), "tp")
    channel_mean = row_sums[0] / channels_all
    channel_var = row_sums[1] / channels_all - channel_mean * channel_mean
    scaled = (conv_out - channel_mean[:, None]) * lax.rsqrt(
        channel_var[:, None] + LN_EPS
    ) * ln_gain[None, :] + ln_bias[None, :]
    mixed_out = jax.nn.silu(scaled).astype(jnp.bfloat16)
    partial_proj = jnp.dot(mixed_out, w_out, preferred_element_type=jnp.float32)
    projected = lax.psum(partial_proj, "tp")
    middle = (resid.astype(jnp.float32) + projected).astype(jnp.bfloat16)
    middle_f = middle.astype(jnp.float32)
    inverse = lax.rsqrt(jnp.mean(middle_f * middle_f, axis=1, keepdims=True) + RMS_EPS)
    normed = (middle_f * inverse * ffn_gain[None, :]).astype(jnp.bfloat16)
    middle_cols = lax.dynamic_slice_in_dim(middle, col_start, col_width, 1)
    shared_gate = jnp.dot(normed, sh_gate, preferred_element_type=jnp.float32)
    shared_up = jnp.dot(normed, sh_up, preferred_element_type=jnp.float32)
    shared_hidden = (jax.nn.silu(shared_gate) * shared_up).astype(jnp.bfloat16)
    weight_rows = sh_down
    shared = jnp.dot(
        lax.all_gather(shared_hidden, "tp", axis=1, tiled=True),
        weight_rows,
        preferred_element_type=jnp.float32,
    )
    top_count = routes.shape[1]
    local_experts = exp_gate.shape[0]
    experts_all = local_experts * sp_count
    capacity = max(2 * tok_rows * top_count // experts_all, tp_count)
    pair_count = tok_rows * top_count
    chosen = routes.reshape(pair_count)
    one_hot = (chosen[:, None] == jnp.arange(experts_all, dtype=jnp.int32)[None, :]).astype(
        jnp.int32
    )
    earlier = jnp.cumsum(one_hot, axis=0) - one_hot
    place_in = jnp.sum(earlier * one_hot, axis=1)
    slot_of = chosen * capacity + place_in
    owner_ids = (
        jnp.zeros((experts_all * capacity,), jnp.int32)
        .at[slot_of]
        .set(jnp.arange(pair_count, dtype=jnp.int32) + 1)
    )
    owner_grid = owner_ids.reshape(sp_count, local_experts, capacity)
    part_slots = capacity // tp_count
    own_owners = lax.dynamic_slice_in_dim(owner_grid, tp_place * part_slots, part_slots, 2)
    source_row = jnp.maximum(own_owners - 1, 0) // top_count
    taken = normed[source_row.reshape(-1)].reshape(own_owners.shape + (model_width,))
    landed = lax.all_to_all(
        jnp.where((own_owners > 0)[..., None], taken, jnp.zeros((), jnp.bfloat16)),
        "sp",
        split_axis=0,
        concat_axis=0,
        tiled=True,
    )
    arrived = lax.all_gather(landed, "tp", axis=2, tiled=True)
    gate_part = jnp.einsum("sxcd,xdf->sxcf", arrived, exp_gate, preferred_element_type=jnp.float32)
    up_part = jnp.einsum("sxcd,xdf->sxcf", arrived, exp_up, preferred_element_type=jnp.float32)
    expert_hidden = (jax.nn.silu(gate_part) * up_part).astype(jnp.bfloat16)
    weight_rows = exp_down
    expert_sum = jnp.einsum(
        "sxcf,xfd->sxcd",
        lax.all_gather(expert_hidden, "tp", axis=3, tiled=True),
        weight_rows,
        preferred_element_type=jnp.float32,
    )
    expert_out = expert_sum.astype(jnp.bfloat16)
    returned = lax.all_to_all(expert_out, "sp", split_axis=0, concat_axis=0, tiled=True)
    flat_out = returned.reshape(experts_all * capacity, col_width)
    picked = flat_out[slot_of].astype(jnp.float32).reshape(tok_rows, top_count, col_width)
    routed = jnp.sum(picked * route_weights[:, :, None], axis=1)
    return (middle_cols.astype(jnp.float32) + shared + routed).astype(jnp.bfloat16)


ROW_CUTS = 2
HALO_PART = 4


def silu(value):
    return value / (1.0 + jnp.exp(-value))


def layer_kernel(
    levels,
    resid_hbm,
    a_val_hbm,
    a_gate_hbm,
    taps_hbm,
    conv_bias_hbm,
    ln_gain_hbm,
    ln_bias_hbm,
    w_out_hbm,
    ffn_gain_hbm,
    routes_hbm,
    route_weights_hbm,
    exp_gate_hbm,
    exp_up_hbm,
    exp_down_hbm,
    sh_gate_hbm,
    sh_up_hbm,
    sh_down_hbm,
    out_ref,
    resid_ref,
    a_val_ref,
    a_gate_ref,
    taps_ref,
    conv_bias_ref,
    ln_gain_ref,
    ln_bias_ref,
    w_out_ref,
    ffn_gain_ref,
    routes_ref,
    route_weights_ref,
    gate_ref,
    up_ref,
    down_ref,
    sh_gate_ref,
    sh_up_ref,
    sh_down_ref,
    halo_out,
    halo_in,
    padded_ref,
    conv_ref,
    stat_out,
    stat_in,
    mix_out,
    mix_in,
    w_in,
    keep_ref,
    chip_out,
    chip_in,
    rows_ref,
    normed_ref,
    hidden_ref,
    shared_ref,
    part_ref,
    back_ref,
    sum_ref,
    weight_ref,
    load_sem,
    halo_sem,
    stat_send,
    stat_recv,
    mix_sem,
    chip_send,
    chip_recv,
    up_sem,
    low_sem,
    side_sem,
    core_sem,
    main_recv,
    core_recv,
    far_send,
    far_recv,
    near_send,
    near_recv,
    relay_send,
    relay_recv,
    shared_send,
    shared_recv,
    back_send,
    back_recv,
):
    count = 2 * levels
    me = lax.axis_index("sp")
    tp_place = lax.axis_index("tp")
    level, side = me // 2, me % 2
    row, core = tp_place // 2, tp_place % 2
    core_place = row * 2 + (1 - core)
    row_place = (1 - row) * 2 + core
    core_peer = {"tp": core_place}
    row_peer = {"tp": row_place}
    far_peer = {"tp": (1 - row) * 2 + (1 - core)}
    side_peer = {"sp": level * 2 + (1 - side)}
    mesh_ids = pl.DeviceIdType.MESH
    f32, bf16 = jnp.float32, jnp.bfloat16
    tok_rows, half_width = resid_ref.shape
    model_width = 2 * half_width
    col_width = out_ref.shape[1]
    span = taps_ref.shape[0]
    halo_rows = halo_in.shape[0]
    channels_all = 4 * a_val_ref.shape[1]
    part_hidden = gate_ref.shape[1]
    cut_rows = tok_rows // ROW_CUTS

    half_at = pl.ds(pl.multiple_of(core * half_width, half_width), half_width)
    pairs = [
        (a_val_hbm, a_val_ref),
        (a_gate_hbm, a_gate_ref),
        (taps_hbm, taps_ref),
        (conv_bias_hbm, conv_bias_ref),
        (ln_gain_hbm, ln_gain_ref),
        (ln_bias_hbm, ln_bias_ref),
        (w_out_hbm.at[:, half_at], w_out_ref),
        (resid_hbm.at[:, half_at], resid_ref),
        (ffn_gain_hbm, ffn_gain_ref),
        (exp_gate_hbm, gate_ref),
        (exp_up_hbm, up_ref),
        (sh_gate_hbm, sh_gate_ref),
        (sh_up_hbm, sh_up_ref),
        (exp_down_hbm, down_ref),
        (sh_down_hbm, sh_down_ref),
        (routes_hbm, routes_ref),
        (route_weights_hbm, route_weights_ref),
    ]
    loads = [
        pltpu.make_async_copy(src, dst, load_sem.at[at]) for at, (src, dst) in enumerate(pairs)
    ]
    for load in loads:
        load.start()

    barrier = pltpu.get_barrier_semaphore()

    def greet(peer):
        pl.semaphore_signal(barrier, inc=1, device_id=peer, device_id_type=mesh_ids)

    across = ((side == 0) & (level > 0)) | ((side == 1) & (level < levels - 1))
    for peer in (core_peer, row_peer, far_peer, side_peer):
        greet(peer)

    @pl.when(level > 0)
    def _():
        greet({"sp": me - 2})

    @pl.when(level < levels - 1)
    def _():
        greet({"sp": me + 2})

    @pl.when(across)
    def _():
        greet({"sp": me + 2 * side - 1})

    def remote(src, dst, send, recv, where):
        return pltpu.make_async_remote_copy(
            src_ref=src, dst_ref=dst, send_sem=send, recv_sem=recv, device_id=where, device_id_type=mesh_ids
        )

    for load in loads[:4]:
        load.wait()
    gated = (a_val_ref[...].astype(f32) / (1.0 + jnp.exp(-a_gate_ref[...].astype(f32)))).astype(bf16)
    halo_out[...] = gated[tok_rows - halo_rows :]
    padded_ref[halo_rows:, :] = gated.astype(f32)
    taps = taps_ref[...].astype(f32)

    def convolve(first, size):
        total = jnp.broadcast_to(conv_bias_ref[...], (size, gated.shape[1]))
        for tap in range(span):
            at = first + tap + halo_rows - (span - 1)
            total = total + taps[tap : tap + 1] * padded_ref[at : at + size, :]
        conv_ref[first : first + size, :] = total

    diagonal = lax.broadcasted_iota(jnp.int32, (tok_rows, tok_rows), 0) == lax.broadcasted_iota(
        jnp.int32, (tok_rows, tok_rows), 1
    )

    def lying(column, first):
        mask = diagonal[first : first + column.shape[0]]
        return jnp.sum(jnp.where(mask, column, 0.0), axis=0, keepdims=True)

    def standing(line, first, size):
        mask = diagonal[first : first + size]
        return jnp.sum(jnp.where(mask, line, 0.0), axis=1, keepdims=True)

    def measure(first, size, part):
        rows = conv_ref[first : first + size, :]
        stat_out[part, 0:1, :] = lying(jnp.sum(rows, axis=1, keepdims=True), first)
        stat_out[part, 1:2, :] = lying(jnp.sum(rows * rows, axis=1, keepdims=True), first)

    stats = [
        [
            remote(
                stat_out.at[part],
                stat_in.at[part, at],
                stat_send.at[part * 3 + at],
                stat_recv.at[part * 3 + at],
                peer,
            )
            for at, peer in enumerate((core_peer, row_peer, far_peer))
        ]
        for part in range(2)
    ]
    rest = tok_rows - halo_rows
    convolve(halo_rows, rest)
    measure(halo_rows, rest, 0)

    has_below = (level + levels - 2) // (levels - 1)
    has_above = (2 * levels - 3 - level) // (levels - 1)
    has_across = has_below + side * (has_above - has_below)
    pl.semaphore_wait(barrier, 4 + has_below + has_above + has_across)
    give_at = pl.ds(pl.multiple_of((1 - core) * half_width, half_width), half_width)
    w_swap = remote(w_out_hbm.at[:, give_at], w_in, mix_sem.at[0], mix_sem.at[1], core_peer)
    halo = lambda where: remote(halo_out, halo_in, halo_sem.at[0], halo_sem.at[1], {"sp": where})

    @pl.when(me < count - 1)
    def _():
        halo(me + 1).start()

    for copy in stats[0]:
        copy.start()
    w_swap.start()

    @pl.when(me == 0)
    def _():
        padded_ref[:halo_rows, :] = jnp.zeros((halo_rows, gated.shape[1]), f32)

    @pl.when(me > 0)
    def _():
        halo(me).wait_recv()
        padded_ref[:halo_rows, :] = halo_in[...].astype(f32)

    convolve(0, halo_rows)
    measure(0, halo_rows, 1)
    for copy in stats[1]:
        copy.start()
    for load in loads[4:9]:
        load.wait()

    def cut(at):
        return pl.ds(at * cut_rows, cut_rows)

    mixes = [
        remote(
            mix_out.at[some], mix_in.at[some], mix_sem.at[2 + part], mix_sem.at[4 + part], core_peer
        )
        for part, some in enumerate((pl.ds(halo_rows, rest), pl.ds(0, halo_rows)))
    ]
    chips = [
        remote(
            chip_out.at[cut(at)], chip_in.at[cut(at)], chip_send.at[at], chip_recv.at[at], row_peer
        )
        for at in range(ROW_CUTS)
    ]

    def project(first, size, part, sending):
        some = slice(first, first + size)
        for copy in stats[part]:
            copy.wait_recv()
        sums = (stat_out[part] + stat_in[part, 0]) + (stat_in[part, 1] + stat_in[part, 2])
        channel_mean = standing(sums[0:1], first, size) / channels_all
        channel_var = standing(sums[1:2], first, size) / channels_all - channel_mean * channel_mean
        scaled = (conv_ref[some, :] - channel_mean) * lax.rsqrt(channel_var + LN_EPS) * ln_gain_ref[
            ...
        ] + ln_bias_ref[...]
        mix_out[some, :] = silu(scaled).astype(bf16)
        mixes[part].start()
        keep_ref[some, :] = jnp.dot(mix_out[some, :], w_out_ref[...], preferred_element_type=f32)
        if part == 0:
            w_swap.wait_recv()
        mixes[part].wait_recv()
        for at in sending:
            chip_sum = keep_ref[cut(at), :] + jnp.dot(
                mix_in[cut(at), :], w_in[...], preferred_element_type=f32
            )
            keep_ref[cut(at), :] = chip_sum
            chip_out[cut(at), :] = chip_sum.astype(bf16)
            chips[at].start()

    project(halo_rows, rest, 0, range(ROW_CUTS - 1, 0, -1))
    project(0, halo_rows, 1, (0,))

    def block(half, at, piece):
        return rows_ref.at[half, at, cut(piece)]

    def up_copy(origin, piece):
        at = origin * 2 + side
        sem = origin * ROW_CUTS + piece
        spot = block(core, at, piece)
        return remote(spot, spot, up_sem.at[sem], main_recv.at[at * ROW_CUTS + piece], {"sp": me + 2})

    def low_copy(origin, piece):
        at = origin * 2 + side
        sem = origin * ROW_CUTS + piece
        spot = block(core, at, piece)
        return remote(spot, spot, low_sem.at[sem], main_recv.at[at * ROW_CUTS + piece], {"sp": me - 2})

    def side_copy(origin, piece):
        at = origin * 2 + side
        sem = origin * ROW_CUTS + piece
        spot = block(core, at, piece)
        return remote(spot, spot, side_sem.at[sem], main_recv.at[at * ROW_CUTS + piece], side_peer)

    def core_copy(at, piece):
        sem = at * ROW_CUTS + piece
        spot = block(core, at, piece)
        return remote(spot, spot, core_sem.at[sem], core_recv.at[sem], core_peer)

    def landed(at, piece):
        spot = block(core, at, piece)
        sem = at * ROW_CUTS + piece
        remote(spot, spot, core_sem.at[sem], main_recv.at[sem], core_peer).wait_recv()

    def crossed(at, piece):
        spot = block(1 - core, at, piece)
        sem = at * ROW_CUTS + piece
        remote(spot, spot, core_sem.at[sem], core_recv.at[sem], core_peer).wait_recv()

    def settle(piece):
        chips[piece].wait_recv()
        total = keep_ref[cut(piece), :] + chip_in[cut(piece), :].astype(f32)
        rows_ref[core, me, cut(piece), :] = (resid_ref[cut(piece), :].astype(f32) + total).astype(bf16)
        core_copy(me, piece).start()
        side_copy(level, piece).start()

        @pl.when(level < levels - 1)
        def _():
            up_copy(level, piece).start()

        @pl.when(level > 0)
        def _():
            low_copy(level, piece).start()

    def normalise(at, some):
        low = rows_ref[0, at, some, :].astype(f32)
        high = rows_ref[1, at, some, :].astype(f32)
        power = jnp.sum(low * low, axis=1, keepdims=True) + jnp.sum(high * high, axis=1, keepdims=True)
        inverse = lax.rsqrt(power / model_width + RMS_EPS)
        normed_ref[some, :half_width] = (low * inverse * ffn_gain_ref[:, :half_width]).astype(bf16)
        normed_ref[some, half_width:] = (high * inverse * ffn_gain_ref[:, half_width:]).astype(bf16)

    def hidden_copy(place, at, run, send, recv, peer):
        spot = hidden_ref.at[place, at, pl.ds(*run)]
        sem = at * ROW_CUTS + run[0] // cut_rows
        return remote(spot, spot, send.at[sem], recv.at[sem], peer)

    def far_copy(at, run):
        return hidden_copy(tp_place, at, run, far_send, far_recv, row_peer)

    def near_copy(at, run):
        return hidden_copy(tp_place, at, run, near_send, near_recv, core_peer)

    def relay_copy(at, run):
        return hidden_copy(row_place, at, run, relay_send, relay_recv, core_peer)

    shared_far = remote(
        shared_ref.at[tp_place], shared_ref.at[tp_place], shared_send.at[0], shared_recv.at[0], row_peer
    )
    shared_near = remote(
        shared_ref.at[tp_place], shared_ref.at[tp_place], shared_send.at[1], shared_recv.at[1], core_peer
    )
    shared_relay = remote(
        shared_ref.at[row_place], shared_ref.at[row_place], shared_send.at[2], shared_recv.at[2], core_peer
    )

    half_rows = tok_rows // 2
    falling = range(ROW_CUTS - 1, -1, -1)
    opening = (half_rows, half_rows)
    closing = (0, half_rows)
    halves = (opening, closing)
    singles = tuple((piece * cut_rows, cut_rows) for piece in falling[: ROW_CUTS // 2])

    def hide(at, first, size, runs):
        some = pl.ds(first, size)
        normalise(at, some)
        step = 256
        for left in range(0, part_hidden, step):
            wide = slice(left, left + step)
            gate_part = jnp.dot(normed_ref[some, :], gate_ref[:, wide], preferred_element_type=f32)
            up_part = jnp.dot(normed_ref[some, :], up_ref[:, wide], preferred_element_type=f32)
            hidden_ref[tp_place, at, some, wide] = (silu(gate_part) * up_part).astype(bf16)
        for run in runs:
            far_copy(at, run).start()
        for run in runs:
            near_copy(at, run).start()

    def gather_hide(at, first, size, runs):
        for piece in range((first + size) // cut_rows - 1, first // cut_rows - 1, -1):
            crossed(at, piece)
        hide(at, first, size, runs)

    def down_part(at, some, place):
        return jnp.dot(
            hidden_ref[place, at, some, :],
            down_ref[pl.ds(pl.multiple_of(place * part_hidden, part_hidden), part_hidden), :],
            preferred_element_type=f32,
        )

    def back_copy(at, half):
        some = pl.ds(half * half_rows, half_rows)
        return remote(
            part_ref.at[at, some],
            back_ref.at[me, some],
            back_send.at[at * 2 + half],
            back_recv.at[me * 2 + half],
            {"sp": at},
        )

    def relay(at, run):
        far_copy(at, run).wait_recv()
        relay_copy(at, run).start()

    def finish(at, first, size, runs):
        for run in runs:
            relay(at, run)
        for run in runs:
            near_copy(at, run).wait_recv()
        for run in runs:
            relay_copy(at, run).wait_recv()
        some = pl.ds(first, size)
        total = (down_part(at, some, 0) + down_part(at, some, 1)) + (
            down_part(at, some, 2) + down_part(at, some, 3)
        )
        part_ref[at, some, :] = total.astype(bf16)
        for half in range((first + size) // half_rows - 1, first // half_rows - 1, -1):
            back_copy(at, half).start()

    def pass_on(step, piece):
        below = level - step
        above = level + step

        @pl.when(below >= 0)
        def _():
            landed(below * 2 + side, piece)

            @pl.when(level < levels - 1)
            def _():
                up_copy(below, piece).start()

            side_copy(below, piece).start()
            core_copy(below * 2 + side, piece).start()

        @pl.when(above < levels)
        def _():
            landed(above * 2 + side, piece)

            @pl.when(level > 0)
            def _():
                low_copy(above, piece).start()

            side_copy(above, piece).start()
            core_copy(above * 2 + side, piece).start()

    def from_side(at):
        for piece in falling:
            landed(at, piece)
            core_copy(at, piece).start()

    upper = (2 * level) // levels
    inner = level + upper * (levels - 1 - 2 * level)

    def visited(outer_way, inner_way):
        mirrored = outer_way[0] + inner * (inner_way[0] - outer_way[0])
        at_level = mirrored + upper * (levels - 1 - 2 * mirrored)
        return at_level * 2 + lax.rem(side + outer_way[1], 2)

    outer_order = ((1, 0), (2, 0), (3, 0), (2, 1), (3, 1), (1, 1))
    inner_order = ((0, 0), (2, 0), (3, 0), (2, 1), (0, 1), (3, 1))
    next_door, *visits = [visited(*ways) for ways in zip(outer_order, inner_order)]
    beside = level * 2 + (1 - side)

    def forward(piece):
        landed(beside, piece)
        core_copy(beside, piece).start()
        pass_on(1, piece)

    settle(falling[0])
    for load in loads[9:11]:
        load.wait()
    gather_hide(me, *opening, (opening,))
    settle(falling[1])
    forward(falling[0])
    gather_hide(next_door, *opening, (opening,))
    forward(falling[1])
    gather_hide(beside, *opening, (opening,))
    gather_hide(next_door, *closing, (closing,))
    for step, at in ((2, visits[0]), (3, visits[1])):
        for piece in falling:
            pass_on(step, piece)
        gather_hide(at, 0, tok_rows, halves)
    for load in loads[11:15]:
        load.wait()
    from_side(visits[2])
    for run in singles:
        relay(me, run)
    finish(next_door, 0, tok_rows, singles + (closing,))
    gather_hide(visits[2], 0, tok_rows, halves)
    from_side(visits[3])
    finish(beside, *opening, (opening,))
    finish(visits[0], 0, tok_rows, halves)
    gather_hide(visits[3], 0, tok_rows, halves)
    from_side(visits[4])
    finish(visits[1], 0, tok_rows, halves)

    for piece in falling[1:]:
        crossed(me, piece)
    whole = pl.ds(0, tok_rows)
    normalise(me, whole)
    shared_gate = jnp.dot(normed_ref[...], sh_gate_ref[...], preferred_element_type=f32)
    shared_up = jnp.dot(normed_ref[...], sh_up_ref[...], preferred_element_type=f32)
    shared_ref[tp_place] = (silu(shared_gate) * shared_up).astype(bf16)
    shared_far.start()
    shared_near.start()

    for load in loads[15:]:
        load.wait()
    for at in range(count):
        line = jnp.sum(
            jnp.where(routes_ref[...] == at, route_weights_ref[...], 0.0), axis=0, keepdims=True
        )
        weight_ref[at] = jnp.broadcast_to(standing(line, 0, tok_rows), weight_ref.shape[1:])

    gather_hide(visits[4], 0, tok_rows, halves)
    finish(visits[2], 0, tok_rows, halves)
    gather_hide(beside, *closing, (closing,))
    hide(me, *closing, (closing,))

    middle_cols = rows_ref[row, me, :, pl.ds(pl.multiple_of(core * col_width, col_width), col_width)]
    shared_far.wait_recv()
    shared_relay.start()
    shared_near.wait_recv()
    shared_relay.wait_recv()
    total = middle_cols.astype(f32)
    shared_width = shared_ref.shape[2]
    for place in range(4):
        total = total + jnp.dot(
            shared_ref[place],
            sh_down_ref[place * shared_width : (place + 1) * shared_width, :],
            preferred_element_type=f32,
        )
    sum_ref[...] = total
    finish(visits[3], 0, tok_rows, halves)
    for half in halves:
        finish(visits[4], *half, (half,))
    finish(beside, *closing, (closing,))

    def add(at, rows):
        weight = jnp.concatenate([weight_ref[at]] * (col_width // weight_ref.shape[2]), axis=1)
        sum_ref[...] += weight * rows.astype(f32)

    def add_back(at):
        for half in range(2):
            some = pl.ds(half * half_rows, half_rows)
            sem = at * 2 + half
            remote(
                part_ref.at[at, some], back_ref.at[at, some], back_send.at[sem], back_recv.at[sem], core_peer
            ).wait_recv()
        add(at, back_ref[at])

    for run in singles + (closing,):
        near_copy(me, run).wait_recv()
    for run in singles:
        relay_copy(me, run).wait_recv()
    own_part = down_part(me, whole, tp_place) + down_part(me, whole, core_place)
    relay(me, closing)
    own_part = own_part + down_part(me, whole, row_place)
    for step in range(2, count):
        add_back(lax.rem(level * 2 + step, count))
    relay_copy(me, closing).wait_recv()
    own_part = own_part + down_part(me, whole, (1 - row) * 2 + (1 - core))
    add(me, own_part.astype(bf16))
    add_back(beside)
    total = sum_ref[...]
    out_ref[...] = total.astype(bf16)

    @pl.when(me < count - 1)
    def _():
        halo(me + 1).wait_send()

    for copy in stats[0] + stats[1] + mixes + chips + [w_swap, shared_far, shared_near, shared_relay]:
        copy.wait_send()

    @pl.loop(0, levels)
    def _(origin):
        for piece in range(ROW_CUTS):
            side_copy(origin, piece).wait_send()

            @pl.when((level < levels - 1) & (origin <= level))
            def _():
                up_copy(origin, piece).wait_send()

            @pl.when((level > 0) & (origin >= level))
            def _():
                low_copy(origin, piece).wait_send()

    split = singles + (closing,)
    trips = [(me, split), (next_door, split), (beside, halves)] + [(at, halves) for at in visits]
    for at, runs in trips:
        for run in runs:
            far_copy(at, run).wait_send()
            near_copy(at, run).wait_send()
            relay_copy(at, run).wait_send()

    @pl.loop(0, count)
    def _(at):
        for piece in range(ROW_CUTS):
            core_copy(at, piece).wait_send()

        @pl.when(at != me)
        def _():
            for half in range(2):
                back_copy(at, half).wait_send()


def body_dense(
    resid,
    a_val,
    a_gate,
    conv_kernel,
    conv_bias,
    ln_gain,
    ln_bias,
    w_out,
    ffn_gain,
    routes,
    route_weights,
    exp_gate,
    exp_up,
    exp_down,
    sh_gate,
    sh_up,
    sh_down,
):
    count = lax.axis_size("sp")
    levels = count // 2
    tok_rows, model_width = resid.shape
    half_width = model_width // 2
    channels = a_val.shape[1]
    part_hidden = exp_gate.shape[2]
    col_width = exp_down.shape[2]
    shared_width = sh_gate.shape[1]
    top_count = routes.shape[1]
    halo_rows = tok_rows // HALO_PART
    vmem = pl.BlockSpec(memory_space=pltpu.VMEM)
    hbm = pl.BlockSpec(memory_space=pltpu.HBM)
    f32, bf16 = jnp.float32, jnp.bfloat16
    dma = pltpu.SemaphoreType.DMA
    operands = (
        resid,
        a_val,
        a_gate,
        conv_kernel,
        conv_bias.reshape(1, -1),
        ln_gain.reshape(1, -1),
        ln_bias.reshape(1, -1),
        w_out,
        ffn_gain.reshape(1, -1),
        routes.T,
        route_weights.T,
        exp_gate[0],
        exp_up[0],
        exp_down[0],
        sh_gate,
        sh_up,
        sh_down,
    )
    pieces = count * ROW_CUTS
    return pl.pallas_call(
        functools.partial(layer_kernel, levels),
        out_shape=jax.ShapeDtypeStruct((tok_rows, col_width), bf16),
        in_specs=[hbm] * len(operands),
        out_specs=vmem,
        scratch_shapes=[
            pltpu.VMEM((tok_rows, half_width), bf16),
            pltpu.VMEM(a_val.shape, bf16),
            pltpu.VMEM(a_gate.shape, bf16),
            pltpu.VMEM(conv_kernel.shape, bf16),
            pltpu.VMEM((1, channels), f32),
            pltpu.VMEM((1, channels), f32),
            pltpu.VMEM((1, channels), f32),
            pltpu.VMEM((channels, half_width), bf16),
            pltpu.VMEM((1, model_width), f32),
            pltpu.VMEM((top_count, tok_rows), jnp.int32),
            pltpu.VMEM((top_count, tok_rows), f32),
            pltpu.VMEM(exp_gate.shape[1:], bf16),
            pltpu.VMEM(exp_up.shape[1:], bf16),
            pltpu.VMEM(exp_down.shape[1:], bf16),
            pltpu.VMEM(sh_gate.shape, bf16),
            pltpu.VMEM(sh_up.shape, bf16),
            pltpu.VMEM(sh_down.shape, bf16),
            pltpu.VMEM((halo_rows, channels), bf16),
            pltpu.VMEM((halo_rows, channels), bf16),
            pltpu.VMEM((halo_rows + tok_rows, channels), f32),
            pltpu.VMEM((tok_rows, channels), f32),
            pltpu.VMEM((2, 2, tok_rows), f32),
            pltpu.VMEM((2, 3, 2, tok_rows), f32),
            pltpu.VMEM((tok_rows, channels), bf16),
            pltpu.VMEM((tok_rows, channels), bf16),
            pltpu.VMEM((channels, half_width), bf16),
            pltpu.VMEM((tok_rows, half_width), f32),
            pltpu.VMEM((tok_rows, half_width), bf16),
            pltpu.VMEM((tok_rows, half_width), bf16),
            pltpu.VMEM((2, count, tok_rows, half_width), bf16),
            pltpu.VMEM((tok_rows, model_width), bf16),
            pltpu.VMEM((4, count, tok_rows, part_hidden), bf16),
            pltpu.VMEM((4, tok_rows, shared_width), bf16),
            pltpu.VMEM((count, tok_rows, col_width), bf16),
            pltpu.VMEM((count, tok_rows, col_width), bf16),
            pltpu.VMEM((tok_rows, col_width), f32),
            pltpu.VMEM((count, tok_rows, 128), f32),
            dma((17,)),
            dma((2,)),
            dma((6,)),
            dma((6,)),
            dma((6,)),
            dma((ROW_CUTS,)),
            dma((ROW_CUTS,)),
            dma((levels * ROW_CUTS,)),
            dma((levels * ROW_CUTS,)),
            dma((levels * ROW_CUTS,)),
            dma((pieces,)),
            dma((pieces,)),
            dma((pieces,)),
            dma((pieces,)),
            dma((pieces,)),
            dma((pieces,)),
            dma((pieces,)),
            dma((pieces,)),
            dma((pieces,)),
            dma((3,)),
            dma((3,)),
            dma((2 * count,)),
            dma((2 * count,)),
        ],
        compiler_params=pltpu.CompilerParams(
            collective_id=0, has_side_effects=True, vmem_limit_bytes=56 * 1024 * 1024
        ),
    )(*operands)


def body(*args):
    tok_rows = args[0].shape[0]
    top_count = args[9].shape[1]
    local_experts = args[11].shape[0]
    experts_all = local_experts * lax.axis_size("sp")
    capacity = 2 * tok_rows * top_count // experts_all
    if (
        local_experts == 1
        and lax.axis_size("tp") == 4
        and lax.axis_size("sp") == 8
        and HALO_PART * (args[3].shape[0] - 1) <= tok_rows
        and capacity >= tok_rows
    ):
        return body_dense(*args)
    return body_slots(*args)


def solution(mesh):
    in_specs = (
        P("sp", None),
        P("sp", "tp"),
        P("sp", "tp"),
        P(None, "tp"),
        P("tp"),
        P("tp"),
        P("tp"),
        P("tp", None),
        P(),
        P("sp", None),
        P("sp", None),
        P("sp", None, "tp"),
        P("sp", None, "tp"),
        P("sp", None, "tp"),
        P(None, "tp"),
        P(None, "tp"),
        P(None, "tp"),
    )
    out_specs = P("sp", "tp")
    return jax.shard_map(body, mesh=mesh, in_specs=in_specs, out_specs=out_specs, check_vma=False)
```
